256 devices in a mesh: sp: 16 (over y, x), tp: 16 (over z, core).
Axes of the slice: x: 4, y: 4, z: 8, core: 2. Of those that a mesh axis runs over, the one named last changes fastest.
Arguments:
- latent: bfloat16 [8192, 4096], P(('sp', 'tp')), may hold values from -6 to 6
- context: bfloat16 [512, 4096], P('sp'), may hold values from -6 to 6
- condition: float32 [4096], replicated, may hold values from -6 to 6
- context_condition: float32 [4096], replicated, may hold values from -6 to 6
- modulation: bfloat16 [3, 4096, 4096], P(None, 'sp', 'tp'), may hold values from -0.09375 to 0.09375
- query_weight: bfloat16 [4096, 4096], P(None, 'tp'), as said below
- key_weight: bfloat16 [4096, 4096], P(None, 'tp'), as said below
- value_weight: bfloat16 [4096, 4096], P(None, 'tp'), may hold values from -0.09375 to 0.09375
- lambdas: float32 [16], P('tp'), may hold values from 0.3 to 0.8
- context_lift: float32 [16], P('tp'), may hold values from 1.5 to 3
- head_gain: float32 [256], replicated, may hold values from 0.1 to 1.9
- output_weight: bfloat16 [4096, 4096], P('tp'), may hold values from -0.09375 to 0.09375
Outputs:
- result: bfloat16 [8192, 4096], P(('sp', 'tp'))
The draws below stay inside these ranges and needn't reach their ends.
Inputs may be any that keep to these rules, and one draw needn't show every extreme that they name: `query_weight`: entries lie within 200 / sqrt(4096) in magnitude. `key_weight`: entries lie within 6 / sqrt(4096) in magnitude.
All inputs are finite; a program needn't handle non-finite values.
Results may differ from the reference program's by a relative error of at most 0.025.
Values may be sent and summed in bfloat16 or wider, within the bound.
A program may use at most 64 MiB of HBM per device.

```python
import math
import jax
import jax.numpy as jnp
from jax import lax

D = 4096
HEADS = 16
HEAD_DIM = 256
GRID_W = 64
CTX = 512
SEQ = 8192


def common_keys(key):
    gaussian = jax.random.normal(jax.random.fold_in(key, 101), (D, HEADS * HEAD_DIM), jnp.float32)
    return jnp.clip(gaussian, -6.0, 6.0) * D ** (-0.5)


def draw_key_weight(key, part):
    return common_keys(key).astype(jnp.bfloat16)


def draw_query_weight(key, part):
    gaussian = jax.random.normal(jax.random.fold_in(key, 202), (D, HEADS * HEAD_DIM), jnp.float32)
    independent = jnp.clip(gaussian, -6.0, 6.0) * D ** (-0.5)
    return independent.astype(jnp.bfloat16)


def steps_of(rng, extent, shards, low, high):
    gain, own = 1.0, jax.random.fold_in(rng, 6)
    for dim, shards_of in shards:
        heights = jnp.exp(jax.random.uniform(jax.random.fold_in(own, dim), (shards_of,), jnp.float32, low / len(shards), high / len(shards)))
        gain = gain * jnp.repeat(heights, extent[dim] // shards_of).reshape([-1 if axis == dim else 1 for axis in range(len(extent))])
    return gain


def scatter_about(own_key, extent, scale, reach, cuts=(), kind=jnp.bfloat16):
    factor_of = steps_of(own_key, extent, cuts, -0.22, 0.18) if cuts else 1.0
    values = jax.random.normal(own_key, extent, jnp.float32) * scale * factor_of
    return jnp.minimum(jnp.maximum(values, -reach), reach).astype(kind)


def setup_inputs(seed: int = 0) -> dict:
    keys = jax.random.split(jax.random.key(seed), 13)
    latent = scatter_about(keys[0], (SEQ, D), 1.0, 6.0, ((0, 256),))
    context = scatter_about(keys[1], (CTX, D), 1.0, 6.0, ((0, 16),))
    condition = scatter_about(keys[2], (D,), 1.0, 6.0, (), jnp.float32)
    context_condition = scatter_about(keys[3], (D,), 1.0, 6.0, (), jnp.float32)
    modulation = scatter_about(keys[4], (3, D, D), D ** -0.5, 0.09375, ((1, 16), (2, 16)))
    query_weight = draw_query_weight(jax.random.fold_in(keys[12], 71), 0)
    key_weight = draw_key_weight(jax.random.fold_in(keys[12], 71), 0)
    value_weight = scatter_about(keys[7], (D, HEADS * HEAD_DIM), D ** -0.5, 0.09375, ((1, 16),))
    lambdas = jnp.clip(0.3 + 0.5 * jax.random.uniform(keys[8], (HEADS,), jnp.float32) ** steps_of(keys[8], (HEADS,), ((0, 16),), -0.2, 0.2), 0.3, 0.8)
    context_lift = jnp.clip(1.5 + 1.5 * jax.random.uniform(keys[9], (HEADS,), jnp.float32) ** steps_of(keys[9], (HEADS,), ((0, 16),), -0.2, 0.2), 1.5, 3.0)
    head_gain = jnp.clip(1.0 + 0.18 * jax.random.normal(keys[10], (HEAD_DIM,), jnp.float32), 0.1, 1.9)
    output_weight = scatter_about(keys[11], (HEADS * HEAD_DIM, D), (HEADS * HEAD_DIM) ** -0.5, 0.09375, ((0, 16),))
    return {"latent": latent, "context": context, "condition": condition, "context_condition": context_condition, "modulation": modulation, "query_weight": query_weight, "key_weight": key_weight, "value_weight": value_weight, "lambdas": lambdas, "context_lift": context_lift, "head_gain": head_gain, "output_weight": output_weight}


ROPE_BASE = 10000.0
EPSILON = 1e-05

def modulate(tokens_in, offset, scaling):
    values = tokens_in.astype(jnp.float32)
    center = lax.optimization_barrier(jnp.mean(values, axis=-1, keepdims=True))
    spread = lax.optimization_barrier(jnp.mean(jnp.square(values - center), axis=-1, keepdims=True))
    normed = (values - center) * lax.rsqrt(spread + EPSILON)
    return (normed * (1.0 + scaling) + offset).astype(jnp.bfloat16)

def rotate(tensor, places):
    number, head_count, head_width = tensor.shape
    quarter = head_width // 4
    eighth = head_width // 8
    inverse = ROPE_BASE ** (-jnp.arange(eighth, dtype=jnp.float32) / eighth)
    grid_row = (places // GRID_W).astype(jnp.float32)
    grid_col = (places % GRID_W).astype(jnp.float32)
    angles = jnp.stack([grid_row[:, None] * inverse, grid_col[:, None] * inverse], axis=1)
    cosine = jnp.cos(angles)[:, None, None, :, :]
    sine_table = jnp.sin(angles)[:, None, None, :, :]
    pieces = tensor.reshape(number, head_count, 2, 2, quarter)
    first_half = pieces[..., :eighth]
    second = pieces[..., eighth:]
    turned = jnp.concatenate([first_half * cosine - second * sine_table, second * cosine + first_half * sine_table], axis=-1)
    return turned.reshape(number, head_count, head_width)

def reference(latent, context, condition, context_condition, modulation, query_weight, key_weight, value_weight, lambdas, context_lift, head_gain, output_weight):
    silu_pair = jax.nn.silu(jnp.stack([condition, context_condition])).astype(jnp.bfloat16)
    mod_vectors = jnp.einsum('cd,rde->cre', silu_pair.astype(jnp.float32), modulation.astype(jnp.float32))
    normed = modulate(latent, mod_vectors[0, 0], mod_vectors[0, 1])
    normed_context = modulate(context, mod_vectors[1, 0], mod_vectors[1, 1])
    seq_len = latent.shape[0]
    half_width = HEAD_DIM // 2
    scale_factor = half_width ** (-0.5)
    query_raw = jnp.dot(normed, query_weight, preferred_element_type=jnp.float32).astype(jnp.bfloat16)
    key_raw = jnp.dot(normed, key_weight, preferred_element_type=jnp.float32).astype(jnp.bfloat16)
    latent_values = jnp.dot(normed, value_weight, preferred_element_type=jnp.float32).astype(jnp.bfloat16)
    context_keys = jnp.dot(normed_context, key_weight, preferred_element_type=jnp.float32).astype(jnp.bfloat16)
    context_values = jnp.dot(normed_context, value_weight, preferred_element_type=jnp.float32).astype(jnp.bfloat16)
    places = jnp.arange(seq_len, dtype=jnp.int32)
    queries = rotate(query_raw.astype(jnp.float32).reshape(seq_len, HEADS, HEAD_DIM), places).astype(jnp.bfloat16)
    latent_keys = rotate(key_raw.astype(jnp.float32).reshape(seq_len, HEADS, HEAD_DIM), places).astype(jnp.bfloat16)
    all_keys = jnp.concatenate([context_keys.reshape(CTX, HEADS, HEAD_DIM), latent_keys], axis=0)
    all_values = jnp.concatenate([context_values.reshape(CTX, HEADS, HEAD_DIM), latent_values.reshape(seq_len, HEADS, HEAD_DIM)], axis=0)
    key_total = CTX + seq_len
    block_len = math.gcd(seq_len, 1024)

    def one_head(inputs):
        head_queries, head_keys, head_values, head_lambda, head_lift = inputs
        lift_row = jnp.where(jnp.arange(key_total) < CTX, head_lift, 0.0)

        def one_block(block_queries):
            outputs = []
            for map_index in range(2):
                low_col = map_index * half_width
                scores = jnp.dot(block_queries[:, low_col:low_col + half_width], head_keys[:, low_col:low_col + half_width].T, preferred_element_type=jnp.float32) * scale_factor + lift_row
                row_peak = lax.optimization_barrier(jnp.max(scores, axis=1, keepdims=True))
                weights = jnp.exp(scores - row_peak)
                row_sums = lax.optimization_barrier(jnp.sum(weights, axis=1, keepdims=True))
                outputs.append(jnp.dot(weights.astype(jnp.bfloat16), head_values, preferred_element_type=jnp.float32) / row_sums)
            difference = outputs[0] - head_lambda * outputs[1]
            scaled = difference * lax.rsqrt(lax.optimization_barrier(jnp.mean(jnp.square(difference), axis=1, keepdims=True)) + EPSILON) * head_gain
            return scaled.astype(jnp.bfloat16)
        blocks = head_queries.reshape(seq_len // block_len, block_len, HEAD_DIM)
        return lax.map(one_block, blocks).reshape(seq_len, HEAD_DIM)
    heads_out = lax.map(one_head, (queries.transpose(1, 0, 2), all_keys.transpose(1, 0, 2), all_values.transpose(1, 0, 2), lambdas, context_lift))
    attended = heads_out.transpose(1, 0, 2).reshape(seq_len, HEADS * HEAD_DIM)
    mixture = jnp.dot(attended, output_weight, preferred_element_type=jnp.float32)
    return (latent.astype(jnp.float32) + mod_vectors[0, 2] * mixture).astype(jnp.bfloat16)
```

```python
import functools

import jax
import jax.numpy as jnp
import numpy as np
from jax import lax
from jax.experimental import pallas as pl
from jax.experimental.pallas import tpu as pltpu
from jax.sharding import PartitionSpec as P

GRID_W = 64
ROPE_BASE = 10000.0
EPSILON = 1e-05
LOG2E = 1.4426950408889634
ROWS = 16
SIDE = 4
VMEM_LIMIT = 63 * 1024 * 1024
MESH = pl.DeviceIdType.MESH
ROW_FIRST = (1, 3, 4)
COLUMN_FIRST = (0, 2)


def aligned(start, size, unit=ROWS):
    return pl.ds(pl.multiple_of(start, unit), size)


def kernel(
    sp_size,
    tp_size,
    latent,
    context,
    condition,
    context_condition,
    modulation,
    query_weight,
    key_weight,
    value_weight,
    row_cos,
    row_sin,
    col_cos,
    col_sin,
    lambdas,
    lift,
    gain,
    output_weight,
    result,
    tokens,
    context_tokens,
    normed,
    mod_weight,
    wq,
    wk,
    wv,
    wo,
    keys_values,
    transit,
    stage,
    queries,
    q_stage,
    peak,
    total_weight,
    mixed,
    attended,
    out_stage,
    mod_parts,
    mod_pieces,
    mod_rows,
    own,
    pair_send,
    pair_recv,
    ring_stage,
    from_left,
    from_right,
    local_sem,
    tok_send,
    tok_recv,
    part_send,
    part_recv,
    piece_send,
    piece_recv,
    kv_send,
    row_recv,
    y_recv,
    y2_recv,
    col_recv,
    x_recv,
    dd_own,
    dd_ownb,
    dd_all,
    q_send,
    q_recv,
    out_send,
    out_recv,
    ps_sem,
    pr_sem,
    st_sem,
    left_sem,
    right_sem,
):
    s = lax.axis_index("sp")
    t = lax.axis_index("tp")
    y = lax.div(s, SIDE)
    x = lax.rem(s, SIDE)
    z = lax.div(t, 2)
    c = lax.rem(t, 2)
    p = lax.rem(x, 2)
    chips = tp_size // 2
    far = chips // 2
    rows, width = latent.shape
    pair = 2 * rows
    block_tokens = tp_size * rows
    ctx_rows = context.shape[0]
    head = query_weight.shape[1]
    half = head // 2
    piece = modulation.shape[2]
    depth = modulation.shape[1]

    def ring(v, n):
        return lax.rem(v + n, n)

    def remote(src, dst, send_sem, recv_sem, sx, sy, sz, sc):
        return pltpu.make_async_remote_copy(
            src_ref=src,
            dst_ref=dst,
            send_sem=send_sem,
            recv_sem=recv_sem,
            device_id={"sp": sy * SIDE + sx, "tp": 2 * sz + sc},
            device_id_type=MESH,
        )

    own_slot = tokens.at[aligned(t * rows, rows)]
    locals_ = [
        pltpu.make_async_copy(src, dst, local_sem.at[i])
        for i, (src, dst) in enumerate(
            [
                (modulation, mod_weight),
                (latent, own_slot),
                (context, context_tokens),
                (key_weight, wk),
                (value_weight, wv),
                (query_weight, wq),
                (output_weight, wo),
            ]
        )
    ]
    for copy in locals_:
        copy.start()

    barrier = pltpu.get_barrier_semaphore()
    for k in range(1, tp_size):
        pl.semaphore_signal(
            barrier, inc=1, device_id={"sp": s, "tp": lax.rem(t + k, tp_size)}, device_id_type=MESH
        )
    for k in range(1, sp_size):
        pl.semaphore_signal(
            barrier, inc=1, device_id={"sp": lax.rem(s + k, sp_size), "tp": t}, device_id_type=MESH
        )
    near = [(1, 0), (2, 0), (3, 0), (0, 1), (0, 3)]
    for dx, dy in near:
        pl.semaphore_signal(
            barrier,
            inc=1,
            device_id={
                "sp": lax.rem(y + dy, SIDE) * SIDE + lax.rem(x + dx, SIDE),
                "tp": 2 * z + 1 - c,
            },
            device_id_type=MESH,
        )

    def silu(ref):
        v = ref[:, aligned(s * depth, depth, 128)]
        return v / (1.0 + jnp.exp(-v))

    first = silu(condition)
    second = silu(context_condition)
    which = lax.broadcasted_iota(jnp.int32, (ROWS, depth), 0)
    vectors = jnp.where(
        which == 0, jnp.broadcast_to(first, (ROWS, depth)), jnp.broadcast_to(second, (ROWS, depth))
    ).astype(jnp.bfloat16)
    locals_[0].wait()
    for r in range(3):
        found = jnp.dot(vectors, mod_weight[r], preferred_element_type=jnp.float32)
        mod_parts[s, 2 * r : 2 * r + 2, :] = found[0:2]
    mod_parts[s, 6:8, :] = jnp.zeros((2, piece), jnp.float32)
    locals_[1].wait()

    pl.semaphore_wait(barrier, tp_size + sp_size - 2 + len(near))

    part_rows = rows // 2

    def token_copy(kind, b, core, part):
        slot = 2 * b + core
        place = tokens.at[aligned(slot * rows + part * part_rows, part_rows)]
        to_z = (ring(z + 1, chips), ring(z - 1, chips), z)[kind]
        return remote(
            place,
            place,
            tok_send.at[kind, 2 * b + part],
            tok_recv.at[2 * slot + part],
            x,
            y,
            to_z,
            1 - c if kind == 2 else c,
        )

    def part_copy(k, owner):
        return pltpu.make_async_remote_copy(
            src_ref=mod_parts.at[owner],
            dst_ref=mod_parts.at[owner],
            send_sem=part_send.at[k],
            recv_sem=part_recv.at[owner],
            device_id={"sp": lax.rem(s + k, sp_size), "tp": t},
            device_id_type=MESH,
        )

    def piece_copy(k, owner):
        return pltpu.make_async_remote_copy(
            src_ref=mod_pieces.at[owner],
            dst_ref=mod_pieces.at[owner],
            send_sem=piece_send.at[k],
            recv_sem=piece_recv.at[owner],
            device_id={"sp": s, "tp": lax.rem(t + k, tp_size)},
            device_id_type=MESH,
        )

    for k in range(1, sp_size):
        part_copy(k, s).start()
    for part in range(2):
        token_copy(0, z, c, part).start()
        token_copy(1, z, c, 1 - part).start()
        token_copy(2, z, c, part).start()

    for k in range(1, sp_size):
        part_copy(k, lax.rem(s + k, sp_size)).wait_recv()
    total = mod_parts[0]
    for i in range(1, sp_size):
        total = total + mod_parts[i]
    mod_pieces[t] = total
    mod_pieces[t, 6:7, :] = jnp.full((1, piece), lambdas[0], jnp.float32)
    mod_pieces[t, 7:8, :] = jnp.full((1, piece), lift[0], jnp.float32)
    for k in range(1, tp_size):
        piece_copy(k, t).start()

    def forward(d, early):
        left = ring(z - d, chips)
        right = ring(z + d, chips)
        right_part, left_part = (0, 1) if early else (1, 0)
        token_copy(2, left, c, right_part).wait_recv()
        if d + 1 < far or (d + 1 == far and early):
            token_copy(0, left, c, right_part).start()
        token_copy(2, left, c, right_part).start()
        token_copy(2, right, c, left_part).wait_recv()
        if d + 1 < far or (d + 1 == far and early):
            token_copy(1, right, c, left_part).start()
        token_copy(2, right, c, left_part).start()

    forward(1, True)
    forward(1, False)
    for k in range(1, tp_size):
        piece_copy(k, lax.rem(t + k, tp_size)).wait_recv()
    for i in range(tp_size):
        mod_rows[:, i * piece : (i + 1) * piece] = mod_pieces[i]

    def normalise(source, base, dest, count, row):
        def group(i, carry):
            v = source[aligned(base + i * ROWS, ROWS), :].astype(jnp.float32)
            v = v - jnp.sum(v, axis=1, keepdims=True) * (1.0 / width)
            spread = jnp.sum(v * v, axis=1, keepdims=True) * (1.0 / width)
            v = v * lax.rsqrt(spread + EPSILON)
            v = v * (1.0 + mod_rows[2 + row : 3 + row, :]) + mod_rows[row : row + 1, :]
            normed[aligned(dest + i * ROWS, ROWS), :] = v.astype(jnp.bfloat16)
            return carry

        lax.fori_loop(0, count // ROWS, group, 0)

    sizes = (ctx_rows + pair, 2 * pair, 2 * pair, 2 * pair, pair)
    starts = tuple(sum(sizes[:g]) for g in range(5))
    q_starts = (0, pair, 3 * pair, 5 * pair, 7 * pair)
    transit_starts = {0: 0, 2: SIDE * sizes[0]}
    halves = tuple(n // 2 for n in sizes)
    own_kind = p == c
    other_kind = p != c
    xs = [x, lax.rem(x + 1, SIDE), lax.rem(x + 2, SIDE), lax.rem(x + 3, SIDE)]
    ys = [y, lax.rem(y + 1, SIDE), lax.rem(y + 2, SIDE), lax.rem(y + 3, SIDE)]

    def kv_at(g, q, sx, sy, count=1):
        order = sy * SIDE + sx if g in ROW_FIRST else sx * SIDE + sy
        n = halves[g]
        return keys_values.at[aligned(sp_size * starts[g] + (q * sp_size + order) * n, count * n)]

    def transit_at(g, q, sy, count=1):
        n = halves[g]
        return transit.at[aligned(transit_starts[g] + (q * SIDE + sy) * n, count * n)]

    def stage_at(g, q):
        return stage.at[aligned(starts[g] + q * halves[g], halves[g])]

    def send(g, k, src, dst, recv_sem, sx, sy, sc):
        return remote(src, dst, kv_send.at[g, k], recv_sem, sx, sy, z, sc)

    def to_partner(g, k, ref, recv_sem=None):
        return send(g, k, ref, ref, dd_all.at[g] if recv_sem is None else recv_sem, x, y, 1 - c)

    def arrived(ref, recv_sem):
        remote(ref, ref, kv_send.at[0, 0], recv_sem, x, y, z, 1 - c).wait_recv()

    def leaving(g, step):
        mine = []
        add = mine.append
        if g in ROW_FIRST:
            i = ROW_FIRST.index(g)
            if step == 1:
                for q in range(2):
                    there = kv_at(g, q, x, y)
                    add((other_kind, send(g, q, stage_at(g, q), there, row_recv.at[i, 2], xs[1], y, q)))
                    add((other_kind, send(g, 2 + q, stage_at(g, q), there, row_recv.at[i, 0], xs[3], y, q)))
                    add((own_kind, send(g, 4 + q, stage_at(g, q), there, row_recv.at[i, 1], xs[2], y, q)))
                add((own_kind, send(g, 6, stage_at(g, 1 - c), kv_at(g, 1 - c, x, y), dd_own.at[g], x, y, 1 - c)))
                add((own_kind, send(g, 7, stage_at(g, c), kv_at(g, c, x, y), dd_ownb.at[g], x, y, 1 - c)))
            if step == 2:
                line = kv_at(g, c, 0, y, SIDE)
                add((None, send(g, 11, line, line, y_recv.at[i, 0], x, ys[1], c)))
                add((None, send(g, 12, line, line, y_recv.at[i, 1], x, ys[3], c)))
                for k in range(3):
                    add((None, to_partner(g, 8 + k, kv_at(g, c, xs[k + 1], y))))
            if step == 3:
                low = kv_at(g, c, 0, ys[3], 2)
                high = kv_at(g, c, 2, ys[1], 2)
                add((None, send(g, 15, low, low, y2_recv.at[i, 0], x, ys[1], c)))
                add((None, send(g, 16, high, high, y2_recv.at[i, 1], x, ys[3], c)))
                add((None, to_partner(g, 13, kv_at(g, c, 0, ys[3], SIDE))))
                add((None, to_partner(g, 14, kv_at(g, c, 0, ys[1], SIDE))))
            if step == 4:
                add((None, to_partner(g, 17, kv_at(g, c, 0, ys[2], SIDE))))
            return mine
        i = COLUMN_FIRST.index(g)
        if step == 1:
            for q in range(2):
                for kind, cond, there in ((0, own_kind, kv_at(g, q, x, y)), (1, other_kind, transit_at(g, q, y))):
                    add((cond, send(g, q, stage_at(g, q), there, col_recv.at[i, 3 * kind], x, ys[1], q)))
                    add((cond, send(g, 2 + q, stage_at(g, q), there, col_recv.at[i, 3 * kind + 1], x, ys[3], q)))
            add((own_kind, send(g, 6, stage_at(g, 1 - c), kv_at(g, 1 - c, x, y), dd_own.at[g], x, y, 1 - c)))
            add((other_kind, send(g, 6, stage_at(g, 1 - c), transit_at(g, 1 - c, y), dd_own.at[g], x, y, 1 - c)))
            add((own_kind, send(g, 7, stage_at(g, c), kv_at(g, c, x, y), dd_ownb.at[g], x, y, 1 - c)))
        if step == 2:
            below = kv_at(g, c, x, ys[3])
            above = transit_at(g, c, ys[1])
            add((None, send(g, 9, below, below, col_recv.at[i, 2], x, ys[1], c)))
            add((None, send(g, 11, above, above, col_recv.at[i, 5], x, ys[3], c)))
            add((None, to_partner(g, 8, below)))
            add((None, to_partner(g, 10, kv_at(g, c, x, ys[1]))))
        if step == 3:
            line = kv_at(g, c, x, 0, SIDE)
            passing = transit_at(g, c, 0, SIDE)
            add((None, send(g, 13, line, line, x_recv.at[i, 1], xs[2], y, c)))
            add((None, send(g, 14, passing, line, x_recv.at[i, 2], xs[1], y, c)))
            add((None, send(g, 15, passing, line, x_recv.at[i, 0], xs[3], y, c)))
            add((None, to_partner(g, 12, kv_at(g, c, x, ys[2]))))
        if step == 4:
            for k in range(3):
                add((None, to_partner(g, 16 + k, kv_at(g, c, xs[k + 1], 0, SIDE))))
        return mine

    def arriving(g, step):
        if g in ROW_FIRST:
            i = ROW_FIRST.index(g)
            if step == 2:
                for k in range(3):
                    arrived(kv_at(g, c, xs[k + 1], y), row_recv.at[i, k])

                @pl.when(other_kind)
                def _():
                    arrived(kv_at(g, c, x, y), dd_own.at[g])

            if step == 3:
                arrived(kv_at(g, c, 0, ys[3], SIDE), y_recv.at[i, 0])
                arrived(kv_at(g, c, 0, ys[1], SIDE), y_recv.at[i, 1])
            if step == 4:
                arrived(kv_at(g, c, 0, ys[2], 2), y2_recv.at[i, 0])
                arrived(kv_at(g, c, 2, ys[2], 2), y2_recv.at[i, 1])
            return
        i = COLUMN_FIRST.index(g)
        if step == 2:
            arrived(kv_at(g, c, x, ys[3]), col_recv.at[i, 0])
            arrived(transit_at(g, c, ys[1]), col_recv.at[i, 4])
            arrived(kv_at(g, c, x, ys[1]), col_recv.at[i, 1])
            arrived(transit_at(g, c, ys[3]), col_recv.at[i, 3])
        if step == 3:
            arrived(kv_at(g, c, x, ys[2]), col_recv.at[i, 2])
            arrived(transit_at(g, c, ys[2]), col_recv.at[i, 5])

            @pl.when(own_kind)
            def _():
                arrived(transit_at(g, c, y), dd_own.at[g])

            @pl.when(other_kind)
            def _():
                arrived(kv_at(g, c, x, y), dd_own.at[g])

        if step == 4:
            for k in range(3):
                arrived(kv_at(g, c, xs[k + 1], 0, SIDE), x_recv.at[i, k])

    def go(copies, wait=False):
        for cond, copy in copies:
            act = copy.wait_send if wait else copy.start
            if cond is None:
                act()
            else:
                pl.when(cond)(act)

    def relay(g, step):
        arriving(g, step)
        go(leaving(g, step))

    def complete(g):
        n = 15 * halves[g]
        arrived(keys_values.at[aligned(sp_size * starts[g], n)], dd_all.at[g])

        @pl.when(other_kind)
        def _():
            arrived(kv_at(g, 1 - c, x, y), dd_ownb.at[g])

    def hand_out(g, keys, values):
        n = halves[g]
        stage[starts[g] : starts[g] + sizes[g], :head] = keys
        stage[starts[g] : starts[g] + sizes[g], head:] = values
        go(leaving(g, 1))

        @pl.when(own_kind)
        def _():
            for q in range(2):
                place = kv_at(g, q, x, y)
                place[:, :head] = keys[q * n : (q + 1) * n]
                place[:, head:] = values[q * n : (q + 1) * n]

        if g in COLUMN_FIRST:
            for q in range(2):

                @pl.when(other_kind & (c == q))
                def _():
                    place = transit_at(g, q, y)
                    place[:, :head] = keys[q * n : (q + 1) * n]
                    place[:, head:] = values[q * n : (q + 1) * n]

    def q_copy(g):
        n = sizes[g] if g else pair
        place = aligned(q_starts[g], n)
        return remote(
            q_stage.at[place],
            queries.at[place],
            q_send.at[g],
            q_recv.at[g],
            x + 1 - 2 * p,
            y,
            z,
            1 - c,
        )

    def hand_query(start, found):
        n = found.shape[0]

        @pl.when(own_kind)
        def _():
            queries[aligned(start, n), :] = found

        @pl.when(other_kind)
        def _():
            q_stage[aligned(start, n), :] = found

    quarter = half // 4
    lane = lax.broadcasted_iota(jnp.int32, (pair, half), 1)
    by_row = lane < half // 2
    low = lax.rem(lax.broadcasted_iota(jnp.int32, (1, half), 1), 2 * quarter) < quarter
    factor = half ** (-0.5) * LOG2E

    def angles(blocks):
        found = []
        for row_table, col_table in ((row_cos, col_cos), (row_sin, col_sin)):
            found.append(
                jnp.concatenate(
                    [
                        jnp.where(by_row, row_table[pl.ds(s * chips + b, 1), :], col_table[...])
                        for b in blocks
                    ],
                    axis=0,
                )
            )
        return found

    def turn(raw, cos, sin, scale=None):
        parts = []
        for i in range(head // half):
            v = raw[:, i * half : (i + 1) * half].astype(jnp.bfloat16).astype(jnp.float32)
            other = jnp.where(low, pltpu.roll(v, half - quarter, 1), pltpu.roll(v, quarter, 1))
            turned = v * cos + other * sin
            if scale is not None:
                turned = turned * scale
            parts.append(turned.astype(jnp.bfloat16))
        return jnp.concatenate(parts, axis=1)

    def from_partner(b):
        for part in range(2):
            token_copy(2, b, 1 - c, part).wait_recv()

    forward(2, True)
    from_partner(z)
    locals_[2].wait()
    normalise(context_tokens, 0, 0, ctx_rows, 1)
    normalise(tokens, z * pair, ctx_rows, pair, 0)
    for i in (3, 4, 5):
        locals_[i].wait()
    cos, sin = angles([z])
    found = jnp.dot(normed[: sizes[0], :], wk[...], preferred_element_type=jnp.float32)
    keys = jnp.concatenate([found[:ctx_rows].astype(jnp.bfloat16), turn(found[ctx_rows:], cos, sin)], axis=0)
    values = jnp.dot(normed[: sizes[0], :], wv[...], preferred_element_type=jnp.float32).astype(jnp.bfloat16)
    hand_out(0, keys, values)
    found = jnp.dot(normed[ctx_rows : sizes[0], :], wq[...], preferred_element_type=jnp.float32)
    hand_query(0, turn(found, cos, sin, factor))
    pl.when(other_kind)(lambda: q_copy(0).start())
    forward(2, False)

    def process(d, carry):
        left = ring(z - d, chips)
        right = ring(z + d, chips)

        @pl.when(d == 3)
        def _():
            forward(3, True)
            forward(3, False)

        from_partner(left)
        from_partner(right)
        normalise(tokens, left * pair, 0, pair, 0)
        normalise(tokens, right * pair, pair, pair, 0)
        cos, sin = angles([left, right])
        v = normed[: 2 * pair, :]
        keys = turn(jnp.dot(v, wk[...], preferred_element_type=jnp.float32), cos, sin)
        values = jnp.dot(v, wv[...], preferred_element_type=jnp.float32).astype(jnp.bfloat16)
        for g in (1, 2, 3):
            pl.when(d == g)(functools.partial(hand_out, g, keys, values))
        found = jnp.dot(v, wq[...], preferred_element_type=jnp.float32)
        hand_query(pair + (d - 1) * 2 * pair, turn(found, cos, sin, factor))
        for g in (1, 2, 3):
            pl.when(other_kind & (d == g))(lambda g=g: q_copy(g).start())

        @pl.when(d == 1)
        def _():
            relay(0, 2)

        @pl.when(d == 2)
        def _():
            relay(0, 3)

        @pl.when(d == 3)
        def _():
            relay(1, 2)

        return carry

    lax.fori_loop(1, 4, process, 0)

    opposite = ring(z + far, chips)
    for part in range(2):
        token_copy(2, opposite, c, part).wait_recv()
        token_copy(2, opposite, c, part).start()
    relay(0, 4)
    from_partner(opposite)
    normalise(tokens, opposite * pair, 0, pair, 0)
    cos, sin = angles([opposite])
    v = normed[:pair, :]
    keys = turn(jnp.dot(v, wk[...], preferred_element_type=jnp.float32), cos, sin)
    values = jnp.dot(v, wv[...], preferred_element_type=jnp.float32).astype(jnp.bfloat16)
    hand_out(4, keys, values)
    found = jnp.dot(v, wq[...], preferred_element_type=jnp.float32)
    hand_query(q_starts[4], turn(found, cos, sin, factor))
    pl.when(other_kind)(lambda: q_copy(4).start())

    relay(1, 3)
    relay(2, 2)

    peak[...] = jnp.full(peak.shape, -jnp.inf, jnp.float32)
    total_weight[...] = jnp.zeros(total_weight.shape, jnp.float32)
    mixed[...] = jnp.zeros(mixed.shape, jnp.float32)

    @pl.when(other_kind)
    def _():
        for g in range(5):
            n = sizes[g] if g else pair
            place = queries.at[aligned(q_starts[g], n)]
            remote(place, place, q_send.at[g], q_recv.at[g], x, y, z, 1 - c).wait_recv()

    my_head = 2 * z + p
    weight_of_second = mod_pieces[my_head, 6:7, 0:1]
    lifted = mod_pieces[my_head, 7:8, 0:1] * LOG2E

    def attend(base, count, first_row, n, raised=None):
        keys_at = aligned(base, count)
        at = slice(first_row, first_row + n)
        scores = [
            lax.dot_general(
                queries[at, m * half : (m + 1) * half],
                keys_values[keys_at, m * half : (m + 1) * half],
                (((1,), (1,)), ((), ())),
                preferred_element_type=jnp.float32,
            )
            for m in range(2)
        ]
        for m in range(2):
            score = scores[m] if raised is None else scores[m] + raised
            old = peak[m, at, :]
            new = jnp.maximum(old, jnp.max(score, axis=1, keepdims=True))
            alpha = jnp.exp2(old - new)
            weights = jnp.exp2(score - new[:, :1])
            total_weight[m, at, :] = total_weight[m, at, :] * alpha + jnp.sum(
                weights, axis=1, keepdims=True
            )
            peak[m, at, :] = new
            mixed[m, at, :] = mixed[m, at, :] * alpha[:, :1] + jnp.dot(
                weights.astype(jnp.bfloat16),
                keys_values[keys_at, head:],
                preferred_element_type=jnp.float32,
            )

    def out_copy(i, first_row, n):
        return remote(
            out_stage.at[first_row : first_row + n],
            attended.at[first_row : first_row + n],
            out_send.at[i],
            out_recv.at[i],
            x + 1 - 2 * p,
            y,
            z,
            1 - c,
        )

    tiles = ((q_starts[3], 3 * pair), (0, q_starts[3]))

    def finish(i):
        first_row, n = tiles[i]
        at = slice(first_row, first_row + n)
        diff = mixed[0, at, :] / total_weight[0, at, :1] - weight_of_second * (
            mixed[1, at, :] / total_weight[1, at, :1]
        )
        mean = jnp.sum(diff * diff, axis=1, keepdims=True) * (1.0 / head)
        found = (diff * lax.rsqrt(mean + EPSILON) * gain[...]).astype(jnp.bfloat16)

        @pl.when(own_kind)
        def _():
            attended[at, :] = found

        @pl.when(other_kind)
        def _():
            out_stage[at, :] = found
            out_copy(i, first_row, n).start()

    complete(0)
    count = sp_size * sizes[0]
    column = lax.broadcasted_iota(jnp.int32, (1, count), 1)
    on_context = (column < count // 2) & (lax.rem(column, halves[0]) < ctx_rows)
    attend(0, count, 0, block_tokens, jnp.where(on_context, lifted, 0.0))
    relay(2, 3)
    relay(1, 4)
    relay(3, 2)

    def groups(g, carry):
        for k in (1, 2, 3):
            pl.when(g == k)(functools.partial(complete, k))
        attend(sp_size * (starts[1] + (g - 1) * sizes[1]), sp_size * sizes[1], 0, block_tokens)

        @pl.when(g == 1)
        def _():
            relay(3, 3)
            relay(2, 4)
            relay(4, 2)

        @pl.when(g == 2)
        def _():
            relay(4, 3)
            relay(3, 4)
            relay(4, 4)

        return carry

    lax.fori_loop(1, 4, groups, 0)
    complete(4)
    locals_[6].wait()
    for i in range(2):
        attend(sp_size * starts[4], sp_size * sizes[4], tiles[i][0], tiles[i][1])
        finish(i)

    span = width // 2
    chunk = 1024

    def pair_copy(u):
        ref = pair_send.at[u]
        return remote(ref, pair_recv.at[u], ps_sem.at[u], pr_sem.at[u], x, y, z, 1 - c)

    def ring_copy(side, d, part):
        u = 2 * d + part
        into = (from_left, from_right)[side]
        sem = (left_sem, right_sem)[side]
        to = (ring(z + 1, chips), ring(z - 1, chips))[side]
        v = 2 * (d - 1) + part
        return remote(
            ring_stage.at[side, u], into.at[v], st_sem.at[side, u], sem.at[v], x, y, to, c
        )

    def ring_arrived(side, d, part):
        v = 2 * d + part
        into = (from_left, from_right)[side]
        sem = (left_sem, right_sem)[side]
        remote(into.at[v], into.at[v], st_sem.at[side, v], sem.at[v], x, y, z, 1 - c).wait_recv()

    def block_of(side, d):
        if d == 0:
            return 0
        if d == far:
            return 2 * far - 1
        return 2 * d if side == 0 else 2 * d - 1

    def compute(d):
        blocks = [block_of(0, d)] if d in (0, far) else [block_of(1, d), block_of(0, d)]
        others = [attended[aligned(j * pair + (1 - c) * rows, rows), :] for j in blocks]
        mines = [attended[aligned(j * pair + c * rows, rows), :] for j in blocks]
        both = jnp.concatenate(others + mines, axis=0)
        n = len(blocks)
        for part in range(2):
            for k in range(span // chunk):
                found = jnp.dot(
                    both,
                    wo[:, part * span + k * chunk : part * span + (k + 1) * chunk],
                    preferred_element_type=jnp.float32,
                )
                cols = slice(k * chunk, (k + 1) * chunk)
                for i, j in enumerate(blocks):
                    pair_send[2 * j + part, :, cols] = found[i * rows : (i + 1) * rows].astype(jnp.bfloat16)
                    own[2 * j + part, :, cols] = found[(n + i) * rows : (n + i + 1) * rows]
            for j in blocks:
                pair_copy(2 * j + part).start()

    def combine(side, d, part):
        u = 2 * block_of(side, d) + part
        pair_copy(u).wait_recv()
        value = own[u] + pair_recv[u].astype(jnp.float32)
        if not (d == far or (d == far - 1 and part != side)):
            ring_arrived(side, d, part)
            value = value + (from_left, from_right)[side][2 * d + part].astype(jnp.float32)
        ring_stage[side, 2 * d + part] = value.astype(jnp.bfloat16)
        ring_copy(side, d, part).start()

    @pl.when(other_kind)
    def _():
        first_row, n = tiles[0]
        out_copy(0, first_row, n).wait_recv()

    compute(4)
    compute(3)
    combine(0, 4, 0)
    combine(1, 4, 1)
    combine(0, 3, 1)
    combine(1, 3, 0)

    @pl.when(other_kind)
    def _():
        first_row, n = tiles[1]
        out_copy(1, first_row, n).wait_recv()

    compute(2)
    combine(0, 3, 0)
    combine(1, 3, 1)
    compute(1)
    for d in (2, 1):
        combine(0, d, 1)
        combine(1, d, 0)
        combine(0, d, 0)
        combine(1, d, 1)
        if d == 2:
            compute(0)

    for part in (1, 0):
        cols = slice(part * span, (part + 1) * span)
        pair_copy(part).wait_recv()
        value = own[part] + pair_recv[part].astype(jnp.float32)
        ring_arrived(0, 0, part)
        value = value + from_left[part].astype(jnp.float32)
        ring_arrived(1, 0, part)
        value = value + from_right[part].astype(jnp.float32)
        result[:, cols] = (
            tokens[aligned(t * rows, rows), cols].astype(jnp.float32) + mod_rows[4:5, cols] * value
        ).astype(jnp.bfloat16)

    for u in range(2 * chips):
        pair_copy(u).wait_send()
    for side in range(2):
        ring_copy(side, far, side).wait_send()
        for d in (1, 2, 3):
            for part in range(2):
                ring_copy(side, d, part).wait_send()
    for part in range(2):
        for d in range(far):
            if d < far - 1 or part == 0:
                token_copy(0, ring(z - d, chips), c, part).wait_send()
            if d < far - 1 or part == 1:
                token_copy(1, ring(z + d, chips), c, part).wait_send()
        for b in range(chips):
            token_copy(2, b, c, part).wait_send()
    for k in range(1, tp_size):
        piece_copy(k, t).wait_send()
    for k in range(1, sp_size):
        part_copy(k, s).wait_send()
    for g in range(5):
        for step in (1, 2, 3, 4):
            go(leaving(g, step), True)

    @pl.when(other_kind)
    def _():
        for g in range(5):
            q_copy(g).wait_send()
        for i in range(2):
            out_copy(i, tiles[i][0], tiles[i][1]).wait_send()


def tables(half):
    quarter = half // 4
    inverse = (ROPE_BASE ** (-np.arange(quarter, dtype=np.float32) / quarter)).astype(np.float32)
    inverse = np.tile(inverse, 4)
    sign = np.where(np.arange(half) % (2 * quarter) < quarter, -1.0, 1.0).astype(np.float32)
    found = []
    for count in (8192 // GRID_W, GRID_W):
        angle = np.arange(count, dtype=np.float32)[:, None] * inverse[None, :]
        found.append(np.cos(angle).astype(np.float32))
        found.append((np.sin(angle) * sign).astype(np.float32))
    return found


def shards(
    sp_size,
    tp_size,
    latent,
    context,
    condition,
    context_condition,
    modulation,
    query_weight,
    key_weight,
    value_weight,
    lambdas,
    context_lift,
    head_gain,
    output_weight,
):
    rows, width = latent.shape
    chips = tp_size // 2
    head = query_weight.shape[1]
    half = head // 2
    pair = 2 * rows
    block_tokens = rows * tp_size
    ctx_rows = context.shape[0]
    piece = modulation.shape[2]
    vmem = pl.BlockSpec(memory_space=pltpu.VMEM)
    smem = pl.BlockSpec(memory_space=pltpu.SMEM)
    anywhere = pl.BlockSpec(memory_space=pl.ANY)
    bf16, f32 = jnp.bfloat16, jnp.float32
    dma = pltpu.SemaphoreType.DMA
    blocks = (2 * chips, rows, width // 2)
    row_cos, row_sin, col_cos, col_sin = tables(half)
    return pl.pallas_call(
        functools.partial(kernel, sp_size, tp_size),
        out_shape=jax.ShapeDtypeStruct((rows, width), bf16),
        in_specs=[anywhere] * 2 + [vmem] * 2 + [anywhere] * 4 + [vmem] * 4 + [smem] * 2 + [vmem, anywhere],
        out_specs=vmem,
        scratch_shapes=[
            pltpu.VMEM((block_tokens, width), bf16),
            pltpu.VMEM(context.shape, bf16),
            pltpu.VMEM((2 * pair, width), bf16),
            pltpu.VMEM(modulation.shape, bf16),
            pltpu.VMEM((width, head), bf16),
            pltpu.VMEM((width, head), bf16),
            pltpu.VMEM((width, head), bf16),
            pltpu.VMEM((head, width), bf16),
            pltpu.VMEM((sp_size * (ctx_rows + block_tokens), 2 * head), bf16),
            pltpu.VMEM((SIDE * (ctx_rows + 3 * pair), 2 * head), bf16),
            pltpu.VMEM((ctx_rows + block_tokens, 2 * head), bf16),
            pltpu.VMEM((block_tokens, head), bf16),
            pltpu.VMEM((block_tokens, head), bf16),
            pltpu.VMEM((2, block_tokens, 128), f32),
            pltpu.VMEM((2, block_tokens, 128), f32),
            pltpu.VMEM((2, block_tokens, head), f32),
            pltpu.VMEM((block_tokens, head), bf16),
            pltpu.VMEM((block_tokens, head), bf16),
            pltpu.VMEM((sp_size, 8, piece), f32),
            pltpu.VMEM((tp_size, 8, piece), f32),
            pltpu.VMEM((8, width), f32),
            pltpu.VMEM(blocks, f32),
            pltpu.VMEM(blocks, bf16),
            pltpu.VMEM(blocks, bf16),
            pltpu.VMEM((2, chips + 2, rows, width // 2), bf16),
            pltpu.VMEM((chips, rows, width // 2), bf16),
            pltpu.VMEM((chips, rows, width // 2), bf16),
            dma((7,)),
            dma((3, 2 * chips)),
            dma((2 * tp_size,)),
            dma((sp_size,)),
            dma((sp_size,)),
            dma((tp_size,)),
            dma((tp_size,)),
            dma((5, 19)),
            dma((3, 3)),
            dma((3, 2)),
            dma((3, 2)),
            dma((2, 6)),
            dma((2, 3)),
            dma((5,)),
            dma((5,)),
            dma((5,)),
            dma((5,)),
            dma((5,)),
            dma((2,)),
            dma((2,)),
            dma((2 * chips,)),
            dma((2 * chips,)),
            dma((2, chips + 2)),
            dma((chips,)),
            dma((chips,)),
        ],
        compiler_params=pltpu.CompilerParams(
            collective_id=0, has_side_effects=True, vmem_limit_bytes=VMEM_LIMIT
        ),
        name="layer",
    )(
        latent,
        context,
        condition.reshape(1, -1),
        context_condition.reshape(1, -1),
        modulation,
        query_weight,
        key_weight,
        value_weight,
        jnp.asarray(row_cos),
        jnp.asarray(row_sin),
        jnp.asarray(col_cos),
        jnp.asarray(col_sin),
        lambdas,
        context_lift,
        head_gain.reshape(1, -1),
        output_weight,
    )


def solution(mesh):
    in_specs = (
        P(("sp", "tp"), None),
        P("sp", None),
        P(),
        P(),
        P(None, "sp", "tp"),
        P(None, "tp"),
        P(None, "tp"),
        P(None, "tp"),
        P("tp"),
        P("tp"),
        P(),
        P("tp", None),
    )
    out_specs = P(("sp", "tp"), None)
    body = functools.partial(shards, mesh.shape["sp"], mesh.shape["tp"])
    return jax.shard_map(body, mesh=mesh, in_specs=in_specs, out_specs=out_specs, check_vma=False)
```

```python
import functools

import jax
import jax.numpy as jnp
import numpy as np
from jax import lax
from jax.experimental import pallas as pl
from jax.experimental.pallas import tpu as pltpu
from jax.sharding import PartitionSpec as P

GRID_W = 64
ROPE_BASE = 10000.0
EPSILON = 1e-05
LOG2E = 1.4426950408889634
ROWS = 16
SIDE = 4
VMEM_LIMIT = 63 * 1024 * 1024
MESH = pl.DeviceIdType.MESH
GROUPS = 5


def aligned(start, size, unit=ROWS):
    return pl.ds(pl.multiple_of(start, unit), size)


def kernel(
    sp_size,
    tp_size,
    latent,
    context,
    condition,
    context_condition,
    modulation,
    query_weight,
    key_weight,
    value_weight,
    row_cos,
    row_sin,
    col_cos,
    col_sin,
    lambdas,
    lift,
    gain,
    output_weight,
    result,
    tokens,
    context_tokens,
    normed,
    mod_weight,
    wq,
    wk,
    wv,
    wo,
    keys_values,
    transit,
    stage,
    queries,
    q_stage,
    peak,
    total_weight,
    mixed,
    attended,
    out_stage,
    mod_parts,
    mod_pieces,
    mod_rows,
    own,
    pair_send,
    pair_recv,
    ring_stage,
    from_left,
    from_right,
    local_sem,
    tok_send,
    tok_recv,
    part_send,
    part_recv,
    piece_send,
    piece_recv,
    kv_send,
    row_recv,
    y_recv,
    y2_recv,
    col_recv,
    x_recv,
    dd_own,
    dd_ownb,
    dd_all,
    q_send,
    q_recv,
    out_send,
    out_recv,
    ps_sem,
    pr_sem,
    st_sem,
    left_sem,
    right_sem,
):
    s = lax.axis_index("sp")
    t = lax.axis_index("tp")
    y = lax.div(s, SIDE)
    x = lax.rem(s, SIDE)
    z = lax.div(t, 2)
    c = lax.rem(t, 2)
    p = lax.rem(x, 2)
    chips = tp_size // 2
    far = chips // 2
    rows, width = latent.shape
    pair = 2 * rows
    block_tokens = tp_size * rows
    ctx_rows = context.shape[0]
    head = query_weight.shape[1]
    half = head // 2
    piece = modulation.shape[2]
    depth = modulation.shape[1]

    def ring(v, n):
        return lax.rem(v + n, n)

    def remote(src, dst, send_sem, recv_sem, sx, sy, sz, sc):
        return pltpu.make_async_remote_copy(
            src_ref=src,
            dst_ref=dst,
            send_sem=send_sem,
            recv_sem=recv_sem,
            device_id={"sp": sy * SIDE + sx, "tp": 2 * sz + sc},
            device_id_type=MESH,
        )

    own_slot = tokens.at[aligned(t * rows, rows)]
    locals_ = [
        pltpu.make_async_copy(src, dst, local_sem.at[i])
        for i, (src, dst) in enumerate(
            [
                (modulation, mod_weight),
                (latent, own_slot),
                (context, context_tokens),
                (key_weight, wk),
                (value_weight, wv),
                (query_weight, wq),
                (output_weight, wo),
            ]
        )
    ]
    for copy in locals_:
        copy.start()

    barrier = pltpu.get_barrier_semaphore()
    for k in range(1, tp_size):
        pl.semaphore_signal(
            barrier, inc=1, device_id={"sp": s, "tp": lax.rem(t + k, tp_size)}, device_id_type=MESH
        )
    for k in range(1, sp_size):
        pl.semaphore_signal(
            barrier, inc=1, device_id={"sp": lax.rem(s + k, sp_size), "tp": t}, device_id_type=MESH
        )
    near = [(1, 0), (2, 0), (3, 0), (0, 1), (0, 3)]
    for dx, dy in near:
        pl.semaphore_signal(
            barrier,
            inc=1,
            device_id={
                "sp": lax.rem(y + dy, SIDE) * SIDE + lax.rem(x + dx, SIDE),
                "tp": 2 * z + 1 - c,
            },
            device_id_type=MESH,
        )

    def silu(ref):
        v = ref[:, aligned(s * depth, depth, 128)]
        return v / (1.0 + jnp.exp(-v))

    first = silu(condition)
    second = silu(context_condition)
    which = lax.broadcasted_iota(jnp.int32, (ROWS, depth), 0)
    vectors = jnp.where(
        which == 0, jnp.broadcast_to(first, (ROWS, depth)), jnp.broadcast_to(second, (ROWS, depth))
    ).astype(jnp.bfloat16)
    locals_[0].wait()
    for r in range(3):
        found = jnp.dot(vectors, mod_weight[r], preferred_element_type=jnp.float32)
        mod_parts[s, 2 * r : 2 * r + 2, :] = found[0:2]
    mod_parts[s, 6:8, :] = jnp.zeros((2, piece), jnp.float32)
    locals_[1].wait()

    pl.semaphore_wait(barrier, tp_size + sp_size - 2 + len(near))

    part_rows = rows // 2

    def token_copy(kind, b, core, part):
        slot = 2 * b + core
        place = tokens.at[aligned(slot * rows + part * part_rows, part_rows)]
        to_z = (ring(z + 1, chips), ring(z - 1, chips), z)[kind]
        return remote(
            place,
            place,
            tok_send.at[kind, 2 * b + part],
            tok_recv.at[2 * slot + part],
            x,
            y,
            to_z,
            1 - c if kind == 2 else c,
        )

    def part_copy(k, owner):
        return pltpu.make_async_remote_copy(
            src_ref=mod_parts.at[owner],
            dst_ref=mod_parts.at[owner],
            send_sem=part_send.at[k],
            recv_sem=part_recv.at[owner],
            device_id={"sp": lax.rem(s + k, sp_size), "tp": t},
            device_id_type=MESH,
        )

    def piece_copy(k, owner):
        return pltpu.make_async_remote_copy(
            src_ref=mod_pieces.at[owner],
            dst_ref=mod_pieces.at[owner],
            send_sem=piece_send.at[k],
            recv_sem=piece_recv.at[owner],
            device_id={"sp": s, "tp": lax.rem(t + k, tp_size)},
            device_id_type=MESH,
        )

    for k in range(1, sp_size):
        part_copy(k, s).start()
    token_copy(0, z, c, 0).start()
    token_copy(1, z, c, 1).start()
    for part in range(2):
        token_copy(2, z, c, part).start()

    for k in range(1, sp_size):
        part_copy(k, lax.rem(s + k, sp_size)).wait_recv()
    total = mod_parts[0]
    for i in range(1, sp_size):
        total = total + mod_parts[i]
    mod_pieces[t] = total
    mod_pieces[t, 6:7, :] = jnp.full((1, piece), lambdas[0], jnp.float32)
    mod_pieces[t, 7:8, :] = jnp.full((1, piece), lift[0], jnp.float32)
    for k in sorted(range(1, tp_size), key=lambda k: -min(k, tp_size - k)):
        piece_copy(k, t).start()
    token_copy(0, z, c, 1).start()
    token_copy(1, z, c, 0).start()

    def forward(d, early):
        left = ring(z - d, chips)
        right = ring(z + d, chips)
        right_part, left_part = (0, 1) if early else (1, 0)
        token_copy(2, left, c, right_part).wait_recv()
        if d + 1 < far or (d + 1 == far and early):
            token_copy(0, left, c, right_part).start()
        token_copy(2, left, c, right_part).start()
        token_copy(2, right, c, left_part).wait_recv()
        if d + 1 < far or (d + 1 == far and early):
            token_copy(1, right, c, left_part).start()
        token_copy(2, right, c, left_part).start()

    forward(1, True)
    for k in range(1, tp_size):
        piece_copy(k, lax.rem(t + k, tp_size)).wait_recv()
    for i in range(tp_size):
        mod_rows[:, i * piece : (i + 1) * piece] = mod_pieces[i]

    def normalise(source, base, dest, count, row):
        v = source[aligned(base, count), :].astype(jnp.float32)
        v = v - jnp.sum(v, axis=1, keepdims=True) * (1.0 / width)
        spread = jnp.sum(v * v, axis=1, keepdims=True) * (1.0 / width)
        v = v * lax.rsqrt(spread + EPSILON)
        v = v * (1.0 + mod_rows[2 + row : 3 + row, :]) + mod_rows[row : row + 1, :]
        normed[aligned(dest, count), :] = v.astype(jnp.bfloat16)

    sizes = (ctx_rows + pair, 2 * pair, 2 * pair, 2 * pair, pair)
    starts = tuple(sum(sizes[:g]) for g in range(GROUPS))
    firsts = (pair, pair, pair, pair, pair // 2)
    halves = tuple((firsts[g], sizes[g] - firsts[g]) for g in range(GROUPS))
    transit_starts = tuple(SIDE * sum(h[1] for h in halves[:g]) for g in range(GROUPS))
    own_kind = p == c
    other_kind = p != c
    xs = [x, lax.rem(x + 1, SIDE), lax.rem(x + 2, SIDE), lax.rem(x + 3, SIDE)]
    ys = [y, lax.rem(y + 1, SIDE), lax.rem(y + 2, SIDE), lax.rem(y + 3, SIDE)]

    def kv_at(g, q, sx, sy, count=1):
        n = halves[g][q]
        order = sx * SIDE + sy if q else sy * SIDE + sx
        start = sp_size * (starts[g] + q * halves[g][0])
        return keys_values.at[aligned(start + order * n, count * n)]

    def transit_at(g, sy, count=1):
        n = halves[g][1]
        return transit.at[aligned(transit_starts[g] + sy * n, count * n)]

    def stage_at(g, q):
        return stage.at[aligned(starts[g] + q * halves[g][0], halves[g][q])]

    def send(g, k, src, dst, recv_sem, sx, sy, sc):
        return remote(src, dst, kv_send.at[g, k], recv_sem, sx, sy, z, sc)

    def to_partner(g, k, ref, recv_sem=None):
        return send(g, k, ref, ref, dd_all.at[g] if recv_sem is None else recv_sem, x, y, 1 - c)

    def arrived(ref, recv_sem):
        remote(ref, ref, kv_send.at[0, 0], recv_sem, x, y, z, 1 - c).wait_recv()

    def leaving(g, step, core=None):
        mine = []

        def add(cond, *args):
            mine.append((cond, send(g, *args)))

        def on(k, ref):
            mine.append((None, to_partner(g, k, ref)))

        if step == 1:
            for q, owner in ((0, 0), (1, 1)):
                here = stage_at(g, q)
                if q == 0:
                    there = kv_at(g, 0, x, y)
                    add(other_kind, 0, here, there, row_recv.at[g, 2], xs[1], y, owner)
                    add(other_kind, 1, here, there, row_recv.at[g, 0], xs[3], y, owner)
                    add(own_kind, 0, here, there, row_recv.at[g, 1], xs[2], y, owner)
                    continue
                for kind, cond, there in ((0, own_kind, kv_at(g, 1, x, y)), (1, other_kind, transit_at(g, y))):
                    add(cond, 2, here, there, col_recv.at[g, 3 * kind], x, ys[1], owner)
                    add(cond, 3, here, there, col_recv.at[g, 3 * kind + 1], x, ys[3], owner)
            for q in range(2):
                cond = own_kind & (c == q)
                add(cond, 4, stage_at(g, 1 - q), kv_at(g, 1 - q, x, y), dd_own.at[g], x, y, 1 - c)
                add(cond, 5, stage_at(g, q), kv_at(g, q, x, y), dd_ownb.at[g], x, y, 1 - c)
            add(other_kind & (c == 0), 4, stage_at(g, 1), transit_at(g, y), dd_own.at[g], x, y, 1 - c)
        elif core == 0:
            if step == 2:
                line = kv_at(g, 0, 0, y, SIDE)
                add(None, 6, line, line, y_recv.at[g, 0], x, ys[1], 0)
                add(None, 7, line, line, y_recv.at[g, 1], x, ys[3], 0)
                for k in range(3):
                    on(8 + k, kv_at(g, 0, xs[k + 1], y))
            if step == 3:
                low = kv_at(g, 0, 0, ys[3], 2)
                high = kv_at(g, 0, 2, ys[1], 2)
                add(None, 11, low, low, y2_recv.at[g, 0], x, ys[1], 0)
                add(None, 12, high, high, y2_recv.at[g, 1], x, ys[3], 0)
                on(13, kv_at(g, 0, 0, ys[3], SIDE))
                on(14, kv_at(g, 0, 0, ys[1], SIDE))
            if step == 4:
                on(15, kv_at(g, 0, 0, ys[2], SIDE))
        else:
            if step == 2:
                below = kv_at(g, 1, x, ys[3])
                above = transit_at(g, ys[1])
                add(None, 6, below, below, col_recv.at[g, 2], x, ys[1], 1)
                add(None, 7, above, above, col_recv.at[g, 5], x, ys[3], 1)
                on(8, below)
                on(9, kv_at(g, 1, x, ys[1]))
            if step == 3:
                line = kv_at(g, 1, x, 0, SIDE)
                passing = transit_at(g, 0, SIDE)
                add(None, 10, line, line, x_recv.at[g, 1], xs[2], y, 1)
                add(None, 11, passing, line, x_recv.at[g, 2], xs[1], y, 1)
                add(None, 12, passing, line, x_recv.at[g, 0], xs[3], y, 1)
                on(13, kv_at(g, 1, x, ys[2]))
            if step == 4:
                for k in range(3):
                    on(14 + k, kv_at(g, 1, xs[k + 1], 0, SIDE))
        return mine

    def arriving(g, step, core):
        if core == 0:
            if step == 2:
                for k in range(3):
                    arrived(kv_at(g, 0, xs[k + 1], y), row_recv.at[g, k])

                @pl.when(other_kind)
                def _():
                    arrived(kv_at(g, 0, x, y), dd_own.at[g])

            if step == 3:
                arrived(kv_at(g, 0, 0, ys[3], SIDE), y_recv.at[g, 0])
                arrived(kv_at(g, 0, 0, ys[1], SIDE), y_recv.at[g, 1])
            if step == 4:
                arrived(kv_at(g, 0, 0, ys[2], 2), y2_recv.at[g, 0])
                arrived(kv_at(g, 0, 2, ys[2], 2), y2_recv.at[g, 1])
            return
        if step == 2:
            arrived(kv_at(g, 1, x, ys[3]), col_recv.at[g, 0])
            arrived(transit_at(g, ys[1]), col_recv.at[g, 4])
            arrived(kv_at(g, 1, x, ys[1]), col_recv.at[g, 1])
            arrived(transit_at(g, ys[3]), col_recv.at[g, 3])
        if step == 3:
            arrived(kv_at(g, 1, x, ys[2]), col_recv.at[g, 2])
            arrived(transit_at(g, ys[2]), col_recv.at[g, 5])

            @pl.when(own_kind)
            def _():
                arrived(transit_at(g, y), dd_own.at[g])

            @pl.when(other_kind)
            def _():
                arrived(kv_at(g, 1, x, y), dd_own.at[g])

        if step == 4:
            for k in range(3):
                arrived(kv_at(g, 1, xs[k + 1], 0, SIDE), x_recv.at[g, k])

    def go(copies, wait=False):
        for cond, copy in copies:
            act = copy.wait_send if wait else copy.start
            if cond is None:
                act()
            else:
                pl.when(cond)(act)

    def relay(core, *stages):
        @pl.when(c == core)
        def _():
            for g, step in stages:
                arriving(g, step, core)
                go(leaving(g, step, core))

    def complete(g):
        for core in range(2):

            @pl.when(c == core)
            def _():
                q = 1 - core
                n = 15 * halves[g][q]
                start = sp_size * (starts[g] + q * halves[g][0])
                arrived(keys_values.at[start : start + n], dd_all.at[g])

                @pl.when(other_kind)
                def _():
                    arrived(kv_at(g, q, x, y), dd_ownb.at[g])

    def hand_out(g, keys, values):
        stage[starts[g] : starts[g] + sizes[g], :head] = keys
        stage[starts[g] : starts[g] + sizes[g], head:] = values
        go(leaving(g, 1))
        parts = (slice(0, halves[g][0]), slice(halves[g][0], sizes[g]))

        @pl.when(own_kind)
        def _():
            for q in range(2):
                place = kv_at(g, q, x, y)
                place[:, :head] = keys[parts[q]]
                place[:, head:] = values[parts[q]]

        @pl.when(other_kind & (c == 1))
        def _():
            place = transit_at(g, y)
            place[:, :head] = keys[parts[1]]
            place[:, head:] = values[parts[1]]

    q_parts = ((0, 5 * pair), (5 * pair, 3 * pair))

    def q_copy(i):
        place = aligned(*q_parts[i])
        return remote(
            q_stage.at[place],
            queries.at[place],
            q_send.at[i],
            q_recv.at[i],
            x + 1 - 2 * p,
            y,
            z,
            1 - c,
        )

    quarter = half // 4
    lane = lax.broadcasted_iota(jnp.int32, (pair, half), 1)
    by_row = lane < half // 2
    low = lax.rem(lax.broadcasted_iota(jnp.int32, (1, half), 1), 2 * quarter) < quarter
    factor = half ** (-0.5) * LOG2E

    def angles(blocks):
        found = []
        for row_table, col_table in ((row_cos, col_cos), (row_sin, col_sin)):
            found.append(
                jnp.concatenate(
                    [
                        jnp.where(by_row, row_table[pl.ds(s * chips + b, 1), :], col_table[...])
                        for b in blocks
                    ],
                    axis=0,
                )
            )
        return found

    def turn(raw, cos, sin, scale=None):
        parts = []
        for i in range(head // half):
            v = raw[:, i * half : (i + 1) * half].astype(jnp.bfloat16).astype(jnp.float32)
            other = jnp.where(low, pltpu.roll(v, half - quarter, 1), pltpu.roll(v, quarter, 1))
            turned = v * cos + other * sin
            if scale is not None:
                turned = turned * scale
            parts.append(turned.astype(jnp.bfloat16))
        return jnp.concatenate(parts, axis=1)

    def from_partner(b):
        for part in range(2):
            token_copy(2, b, 1 - c, part).wait_recv()

    def ask(i, blocks):
        first_row, n = q_parts[i]
        at = slice(first_row, first_row + n)
        cos, sin = angles(blocks)
        found = jnp.dot(
            normed[ctx_rows + first_row : ctx_rows + first_row + n, :],
            wq[...],
            preferred_element_type=jnp.float32,
        )
        found = turn(found, cos, sin, factor)

        @pl.when(own_kind)
        def _():
            queries[at, :] = found

        @pl.when(other_kind)
        def _():
            q_stage[at, :] = found
            q_copy(i).start()

    from_partner(z)
    locals_[2].wait()
    normalise(context_tokens, 0, 0, ctx_rows, 1)
    normalise(tokens, z * pair, ctx_rows, pair, 0)
    for i in (3, 4, 5):
        locals_[i].wait()
    cos, sin = angles([z])
    found = jnp.dot(normed[: sizes[0], :], wk[...], preferred_element_type=jnp.float32)
    keys = jnp.concatenate([found[:ctx_rows].astype(jnp.bfloat16), turn(found[ctx_rows:], cos, sin)], axis=0)
    values = jnp.dot(normed[: sizes[0], :], wv[...], preferred_element_type=jnp.float32).astype(jnp.bfloat16)
    hand_out(0, keys, values)
    forward(1, False)

    def process(d, carry):
        left = ring(z - d, chips)
        right = ring(z + d, chips)

        from_partner(left)
        from_partner(right)
        base = starts[1] + (d - 1) * 2 * pair
        normalise(tokens, left * pair, base, pair, 0)
        normalise(tokens, right * pair, base + pair, pair, 0)

        @pl.when(d == 1)
        def _():
            forward(2, True)

        @pl.when(d == 2)
        def _():
            forward(3, True)
            relay(0, (0, 2))
            relay(1, (0, 2))

        @pl.when(d == 3)
        def _():
            opposite = ring(z + far, chips)
            token_copy(2, opposite, c, 0).wait_recv()
            token_copy(2, opposite, c, 0).start()
            relay(0, (1, 2))
            relay(1, (1, 2), (0, 3))

        cos, sin = angles([left, right])
        v = normed[aligned(base, 2 * pair), :]
        keys = turn(jnp.dot(v, wk[...], preferred_element_type=jnp.float32), cos, sin)
        values = jnp.dot(v, wv[...], preferred_element_type=jnp.float32).astype(jnp.bfloat16)
        for g in (1, 2, 3):
            pl.when(d == g)(functools.partial(hand_out, g, keys, values))

        @pl.when(d == 1)
        def _():
            forward(2, False)

        @pl.when(d == 2)
        def _():
            around = [z]
            for k in (1, 2):
                around += [ring(z - k, chips), ring(z + k, chips)]
            ask(0, around)
            forward(3, False)

        return carry

    lax.fori_loop(1, 4, process, 0)

    opposite = ring(z + far, chips)
    token_copy(2, opposite, c, 1).wait_recv()
    token_copy(2, opposite, c, 1).start()
    relay(0, (2, 2))
    from_partner(opposite)
    normalise(tokens, opposite * pair, starts[4], pair, 0)
    relay(1, (2, 2))
    cos, sin = angles([opposite])
    v = normed[starts[4] : starts[4] + pair, :]
    keys = turn(jnp.dot(v, wk[...], preferred_element_type=jnp.float32), cos, sin)
    values = jnp.dot(v, wv[...], preferred_element_type=jnp.float32).astype(jnp.bfloat16)
    hand_out(4, keys, values)
    relay(0, (0, 3))
    relay(1, (1, 3))
    ask(1, [ring(z - 3, chips), ring(z + 3, chips), opposite])
    relay(0, (3, 2), (4, 2), (1, 3), (2, 3), (0, 4))
    relay(1, (3, 2), (0, 4), (2, 3), (4, 2), (3, 3), (4, 3))

    peak[...] = jnp.full(peak.shape, -jnp.inf, jnp.float32)
    total_weight[...] = jnp.zeros(total_weight.shape, jnp.float32)
    mixed[...] = jnp.zeros(mixed.shape, jnp.float32)

    @pl.when(other_kind)
    def _():
        for i in range(2):
            place = queries.at[aligned(*q_parts[i])]
            remote(place, place, q_send.at[i], q_recv.at[i], x, y, z, 1 - c).wait_recv()

    my_head = 2 * z + p
    weight_of_second = mod_pieces[my_head, 6:7, 0:1]
    lifted = mod_pieces[my_head, 7:8, 0:1] * LOG2E

    def attend(base, count, first_row, n, raised=None):
        keys_at = aligned(base, count)
        at = aligned(first_row, n)
        scores = [
            lax.dot_general(
                queries[at, m * half : (m + 1) * half],
                keys_values[keys_at, m * half : (m + 1) * half],
                (((1,), (1,)), ((), ())),
                preferred_element_type=jnp.float32,
            )
            for m in range(2)
        ]
        for m in range(2):
            score = scores[m] if raised is None else scores[m] + raised
            old = peak[m, at, :]
            new = jnp.maximum(old, jnp.max(score, axis=1, keepdims=True))
            alpha = jnp.exp2(old - new)
            weights = jnp.exp2(score - new[:, :1])
            total_weight[m, at, :] = total_weight[m, at, :] * alpha + jnp.sum(
                weights, axis=1, keepdims=True
            )
            peak[m, at, :] = new
            mixed[m, at, :] = mixed[m, at, :] * alpha[:, :1] + jnp.dot(
                weights.astype(jnp.bfloat16),
                keys_values[keys_at, head:],
                preferred_element_type=jnp.float32,
            )

    def out_copy(i, first_row, n):
        return remote(
            out_stage.at[first_row : first_row + n],
            attended.at[first_row : first_row + n],
            out_send.at[i],
            out_recv.at[i],
            x + 1 - 2 * p,
            y,
            z,
            1 - c,
        )

    tiles = (q_parts[1], q_parts[0])

    def finish(i):
        first_row, n = tiles[i]
        at = slice(first_row, first_row + n)
        diff = mixed[0, at, :] / total_weight[0, at, :1] - weight_of_second * (
            mixed[1, at, :] / total_weight[1, at, :1]
        )
        mean = jnp.sum(diff * diff, axis=1, keepdims=True) * (1.0 / head)
        found = (diff * lax.rsqrt(mean + EPSILON) * gain[...]).astype(jnp.bfloat16)

        @pl.when(own_kind)
        def _():
            attended[at, :] = found

        @pl.when(other_kind)
        def _():
            out_stage[at, :] = found
            out_copy(i, first_row, n).start()

    count = sp_size * sizes[0]
    column = lax.broadcasted_iota(jnp.int32, (1, count), 1)
    on_context = (column < sp_size * halves[0][0]) & (lax.rem(column, halves[0][0]) < ctx_rows)
    raised = jnp.where(on_context, lifted, 0.0)
    tile = block_tokens // 2

    complete(0)

    def first_group(i, carry):
        attend(0, count, i * tile, tile, raised)

        @pl.when(i == 0)
        def _():
            relay(0, (3, 3))

        return carry

    lax.fori_loop(0, 2, first_group, 0)
    relay(0, (4, 3), (1, 4))
    relay(1, (1, 4))
    complete(1)

    def groups(j, carry):
        g = lax.div(j, 2) + 1
        i = lax.rem(j, 2)
        attend(sp_size * (starts[1] + (g - 1) * sizes[1]), sp_size * sizes[1], i * tile, tile)

        @pl.when(j == 0)
        def _():
            relay(0, (2, 4))
            relay(1, (2, 4))

        @pl.when(j == 1)
        def _():
            complete(2)

        @pl.when(j == 2)
        def _():
            relay(0, (3, 4), (4, 4))
            relay(1, (3, 4))

        @pl.when(j == 3)
        def _():
            relay(1, (4, 4))
            complete(3)

        return carry

    lax.fori_loop(0, 6, groups, 0)
    complete(4)
    locals_[6].wait()

    def last_group(i):
        attend(sp_size * starts[4], sp_size * sizes[4], tiles[i][0], tiles[i][1])
        finish(i)

    last_group(0)
    last_group(1)

    span = width // 2
    chunk = 1024

    def pair_copy(u):
        ref = pair_send.at[u]
        return remote(ref, pair_recv.at[u], ps_sem.at[u], pr_sem.at[u], x, y, z, 1 - c)

    def ring_copy(side, d, part):
        u = 2 * d + part
        into = (from_left, from_right)[side]
        sem = (left_sem, right_sem)[side]
        to = (ring(z + 1, chips), ring(z - 1, chips))[side]
        v = 2 * (d - 1) + part
        return remote(
            ring_stage.at[side, u], into.at[v], st_sem.at[side, u], sem.at[v], x, y, to, c
        )

    def ring_arrived(side, d, part):
        v = 2 * d + part
        into = (from_left, from_right)[side]
        sem = (left_sem, right_sem)[side]
        remote(into.at[v], into.at[v], st_sem.at[side, v], sem.at[v], x, y, z, 1 - c).wait_recv()

    def block_of(side, d):
        if d == 0:
            return 0
        if d == far:
            return 2 * far - 1
        return 2 * d if side == 0 else 2 * d - 1

    def compute(d):
        blocks = [block_of(0, d)] if d in (0, far) else [block_of(1, d), block_of(0, d)]
        others = [attended[aligned(j * pair + (1 - c) * rows, rows), :] for j in blocks]
        mines = [attended[aligned(j * pair + c * rows, rows), :] for j in blocks]
        both = jnp.concatenate(others + mines, axis=0)
        n = len(blocks)
        for part in range(2):
            for k in range(span // chunk):
                found = jnp.dot(
                    both,
                    wo[:, part * span + k * chunk : part * span + (k + 1) * chunk],
                    preferred_element_type=jnp.float32,
                )
                cols = slice(k * chunk, (k + 1) * chunk)
                for i, j in enumerate(blocks):
                    pair_send[2 * j + part, :, cols] = found[i * rows : (i + 1) * rows].astype(jnp.bfloat16)
                    own[2 * j + part, :, cols] = found[(n + i) * rows : (n + i + 1) * rows]
            for j in blocks:
                pair_copy(2 * j + part).start()

    def combine(side, d, part):
        u = 2 * block_of(side, d) + part
        pair_copy(u).wait_recv()
        value = own[u] + pair_recv[u].astype(jnp.float32)
        if not (d == far or (d == far - 1 and part != side)):
            ring_arrived(side, d, part)
            value = value + (from_left, from_right)[side][2 * d + part].astype(jnp.float32)
        ring_stage[side, 2 * d + part] = value.astype(jnp.bfloat16)
        ring_copy(side, d, part).start()

    @pl.when(other_kind)
    def _():
        first_row, n = tiles[0]
        out_copy(0, first_row, n).wait_recv()

    compute(4)
    combine(0, 4, 0)
    combine(1, 4, 1)
    compute(3)
    combine(0, 3, 1)
    combine(1, 3, 0)
    combine(0, 3, 0)
    combine(1, 3, 1)

    @pl.when(other_kind)
    def _():
        first_row, n = tiles[1]
        out_copy(1, first_row, n).wait_recv()

    compute(2)
    combine(0, 2, 1)
    combine(1, 2, 0)
    compute(1)

    for part in range(2):
        for d in range(far):
            if d < far - 1 or part == 0:
                token_copy(0, ring(z - d, chips), c, part).wait_send()
            if d < far - 1 or part == 1:
                token_copy(1, ring(z + d, chips), c, part).wait_send()
        for b in range(chips):
            token_copy(2, b, c, part).wait_send()
    for k in range(1, tp_size):
        piece_copy(k, t).wait_send()
    for k in range(1, sp_size):
        part_copy(k, s).wait_send()
    combine(0, 2, 0)
    combine(1, 2, 1)
    compute(0)
    for g in range(GROUPS):
        go(leaving(g, 1), True)
    for core in range(2):

        @pl.when(c == core)
        def _():
            for g in range(GROUPS):
                for step in (2, 3, 4):
                    go(leaving(g, step, core), True)

    @pl.when(other_kind)
    def _():
        for i in range(2):
            q_copy(i).wait_send()
            out_copy(i, tiles[i][0], tiles[i][1]).wait_send()

    for u in range(2 * chips):
        pair_copy(u).wait_send()
    combine(0, 1, 1)
    combine(1, 1, 0)
    combine(0, 1, 0)
    combine(1, 1, 1)

    for part in (1, 0):
        cols = slice(part * span, (part + 1) * span)
        pair_copy(part).wait_recv()
        value = own[part] + pair_recv[part].astype(jnp.float32)
        ring_arrived(0, 0, part)
        value = value + from_left[part].astype(jnp.float32)
        ring_arrived(1, 0, part)
        value = value + from_right[part].astype(jnp.float32)
        result[:, cols] = (
            tokens[aligned(t * rows, rows), cols].astype(jnp.float32) + mod_rows[4:5, cols] * value
        ).astype(jnp.bfloat16)

    for side in range(2):
        ring_copy(side, far, side).wait_send()
        for d in (1, 2, 3):
            for part in range(2):
                ring_copy(side, d, part).wait_send()


def tables(half):
    quarter = half // 4
    inverse = (ROPE_BASE ** (-np.arange(quarter, dtype=np.float32) / quarter)).astype(np.float32)
    inverse = np.tile(inverse, 4)
    sign = np.where(np.arange(half) % (2 * quarter) < quarter, -1.0, 1.0).astype(np.float32)
    found = []
    for count in (8192 // GRID_W, GRID_W):
        angle = np.arange(count, dtype=np.float32)[:, None] * inverse[None, :]
        found.append(np.cos(angle).astype(np.float32))
        found.append((np.sin(angle) * sign).astype(np.float32))
    return found


def shards(
    sp_size,
    tp_size,
    latent,
    context,
    condition,
    context_condition,
    modulation,
    query_weight,
    key_weight,
    value_weight,
    lambdas,
    context_lift,
    head_gain,
    output_weight,
):
    rows, width = latent.shape
    chips = tp_size // 2
    head = query_weight.shape[1]
    half = head // 2
    pair = 2 * rows
    block_tokens = rows * tp_size
    ctx_rows = context.shape[0]
    piece = modulation.shape[2]
    vmem = pl.BlockSpec(memory_space=pltpu.VMEM)
    smem = pl.BlockSpec(memory_space=pltpu.SMEM)
    anywhere = pl.BlockSpec(memory_space=pl.ANY)
    bf16, f32 = jnp.bfloat16, jnp.float32
    dma = pltpu.SemaphoreType.DMA
    blocks = (2 * chips, rows, width // 2)
    row_cos, row_sin, col_cos, col_sin = tables(half)
    return pl.pallas_call(
        functools.partial(kernel, sp_size, tp_size),
        out_shape=jax.ShapeDtypeStruct((rows, width), bf16),
        in_specs=[anywhere] * 2 + [vmem] * 2 + [anywhere] * 4 + [vmem] * 4 + [smem] * 2 + [vmem, anywhere],
        out_specs=vmem,
        scratch_shapes=[
            pltpu.VMEM((block_tokens, width), bf16),
            pltpu.VMEM(context.shape, bf16),
            pltpu.VMEM((ctx_rows + block_tokens, width), bf16),
            pltpu.VMEM(modulation.shape, bf16),
            pltpu.VMEM((width, head), bf16),
            pltpu.VMEM((width, head), bf16),
            pltpu.VMEM((width, head), bf16),
            pltpu.VMEM((head, width), bf16),
            pltpu.VMEM((sp_size * (ctx_rows + block_tokens), 2 * head), bf16),
            pltpu.VMEM((SIDE * block_tokens // 2, 2 * head), bf16),
            pltpu.VMEM((ctx_rows + block_tokens, 2 * head), bf16),
            pltpu.VMEM((block_tokens, head), bf16),
            pltpu.VMEM((block_tokens, head), bf16),
            pltpu.VMEM((2, block_tokens, 128), f32),
            pltpu.VMEM((2, block_tokens, 128), f32),
            pltpu.VMEM((2, block_tokens, head), f32),
            pltpu.VMEM((block_tokens, head), bf16),
            pltpu.VMEM((block_tokens, head), bf16),
            pltpu.VMEM((sp_size, 8, piece), f32),
            pltpu.VMEM((tp_size, 8, piece), f32),
            pltpu.VMEM((8, width), f32),
            pltpu.VMEM(blocks, f32),
            pltpu.VMEM(blocks, bf16),
            pltpu.VMEM(blocks, bf16),
            pltpu.VMEM((2, chips + 2, rows, width // 2), bf16),
            pltpu.VMEM((chips, rows, width // 2), bf16),
            pltpu.VMEM((chips, rows, width // 2), bf16),
            dma((7,)),
            dma((3, 2 * chips)),
            dma((2 * tp_size,)),
            dma((sp_size,)),
            dma((sp_size,)),
            dma((tp_size,)),
            dma((tp_size,)),
            dma((5, 17)),
            dma((5, 3)),
            dma((5, 2)),
            dma((5, 2)),
            dma((5, 6)),
            dma((5, 3)),
            dma((5,)),
            dma((5,)),
            dma((5,)),
            dma((2,)),
            dma((2,)),
            dma((2,)),
            dma((2,)),
            dma((2 * chips,)),
            dma((2 * chips,)),
            dma((2, chips + 2)),
            dma((chips,)),
            dma((chips,)),
        ],
        compiler_params=pltpu.CompilerParams(
            collective_id=0, has_side_effects=True, vmem_limit_bytes=VMEM_LIMIT
        ),
        name="layer",
    )(
        latent,
        context,
        condition.reshape(1, -1),
        context_condition.reshape(1, -1),
        modulation,
        query_weight,
        key_weight,
        value_weight,
        jnp.asarray(row_cos),
        jnp.asarray(row_sin),
        jnp.asarray(col_cos),
        jnp.asarray(col_sin),
        lambdas,
        context_lift,
        head_gain.reshape(1, -1),
        output_weight,
    )


def solution(mesh):
    in_specs = (
        P(("sp", "tp"), None),
        P("sp", None),
        P(),
        P(),
        P(None, "sp", "tp"),
        P(None, "tp"),
        P(None, "tp"),
        P(None, "tp"),
        P("tp"),
        P("tp"),
        P(),
        P("tp", None),
    )
    out_specs = P(("sp", "tp"), None)
    body = functools.partial(shards, mesh.shape["sp"], mesh.shape["tp"])
    return jax.shard_map(body, mesh=mesh, in_specs=in_specs, out_specs=out_specs, check_vma=False)
```

```python
import functools

import jax
import jax.numpy as jnp
import numpy as np
from jax import lax
from jax.experimental import pallas as pl
from jax.experimental.pallas import tpu as pltpu
from jax.sharding import PartitionSpec as P

GRID_W = 64
ROPE_BASE = 10000.0
EPSILON = 1e-05
LOG2E = 1.4426950408889634
ROWS = 16
SIDE = 4
VMEM_LIMIT = 63 * 1024 * 1024
MESH = pl.DeviceIdType.MESH
GROUPS = 5


def aligned(start, size, unit=ROWS):
    return pl.ds(pl.multiple_of(start, unit), size)


def kernel(
    sp_size,
    tp_size,
    latent,
    context,
    condition,
    context_condition,
    modulation,
    query_weight,
    key_weight,
    value_weight,
    row_cos,
    row_sin,
    col_cos,
    col_sin,
    lambdas,
    lift,
    gain,
    output_weight,
    result,
    tokens,
    context_tokens,
    normed,
    mod_weight,
    wq,
    wk,
    wv,
    wo,
    keys_values,
    transit,
    stage,
    queries,
    q_stage,
    peak,
    total_weight,
    mixed,
    attended,
    out_stage,
    mod_parts,
    mod_pieces,
    mod_rows,
    own,
    pair_send,
    pair_recv,
    ring_stage,
    from_left,
    from_right,
    handed,
    local_sem,
    tok_send,
    tok_recv,
    part_sem,
    piece_sem,
    kv_send,
    stage_recv,
    dd_own,
    dd_ownb,
    dd_all,
    q_sem,
    out_sem,
    ps_sem,
    pr_sem,
    st_sem,
    left_sem,
    right_sem,
):
    s = lax.axis_index("sp")
    t = lax.axis_index("tp")
    y = lax.div(s, SIDE)
    x = lax.rem(s, SIDE)
    z = lax.div(t, 2)
    c = lax.rem(t, 2)
    p = lax.rem(x, 2)
    chips = tp_size // 2
    far = chips // 2
    rows, width = latent.shape
    pair = 2 * rows
    block_tokens = tp_size * rows
    ctx_rows = context.shape[0]
    head = query_weight.shape[1]
    half = head // 2
    piece = modulation.shape[2]
    depth = modulation.shape[1]

    def ring(v, n):
        return lax.rem(v + n, n)

    def awaited(ref, sem):
        pltpu.make_async_copy(ref, ref, sem).wait()

    def remote(src, dst, send_sem, recv_sem, sx, sy, sz, sc):
        return pltpu.make_async_remote_copy(
            src_ref=src,
            dst_ref=dst,
            send_sem=send_sem,
            recv_sem=recv_sem,
            device_id={"sp": sy * SIDE + sx, "tp": 2 * sz + sc},
            device_id_type=MESH,
        )

    own_slot = tokens.at[aligned(t * rows, rows)]
    locals_ = [
        pltpu.make_async_copy(src, dst, local_sem.at[i])
        for i, (src, dst) in enumerate(
            [
                (modulation, mod_weight),
                (latent, own_slot),
                (context, context_tokens),
                (key_weight, wk),
                (value_weight, wv),
                (query_weight, wq),
                (output_weight, wo),
            ]
        )
    ]
    for copy in locals_:
        copy.start()

    barrier = pltpu.get_barrier_semaphore()
    for k in range(1, tp_size):
        pl.semaphore_signal(
            barrier, inc=1, device_id={"sp": s, "tp": lax.rem(t + k, tp_size)}, device_id_type=MESH
        )
    for k in range(1, sp_size):
        pl.semaphore_signal(
            barrier, inc=1, device_id={"sp": lax.rem(s + k, sp_size), "tp": t}, device_id_type=MESH
        )
    near = [(1, 0), (2, 0), (3, 0), (0, 1), (0, 3)]
    for dx, dy in near:
        pl.semaphore_signal(
            barrier,
            inc=1,
            device_id={
                "sp": lax.rem(y + dy, SIDE) * SIDE + lax.rem(x + dx, SIDE),
                "tp": 2 * z + 1 - c,
            },
            device_id_type=MESH,
        )

    def silu(ref):
        v = ref[:, aligned(s * depth, depth, 128)]
        return v / (1.0 + jnp.exp(-v))

    first = silu(condition)
    second = silu(context_condition)
    which = lax.broadcasted_iota(jnp.int32, (ROWS, depth), 0)
    vectors = jnp.where(
        which == 0, jnp.broadcast_to(first, (ROWS, depth)), jnp.broadcast_to(second, (ROWS, depth))
    ).astype(jnp.bfloat16)
    locals_[0].wait()
    for r in range(3):
        found = jnp.dot(vectors, mod_weight[r], preferred_element_type=jnp.float32)
        mod_parts[s, 2 * r : 2 * r + 2, :] = found[0:2]
    mod_parts[s, 6:8, :] = jnp.zeros((2, piece), jnp.float32)
    locals_[1].wait()

    pl.semaphore_wait(barrier, tp_size + sp_size - 2 + len(near))

    part_rows = rows // 2

    def token_copy(kind, b, core, part):
        slot = 2 * b + core
        place = tokens.at[aligned(slot * rows + part * part_rows, part_rows)]
        to_z = (ring(z + 1, chips), ring(z - 1, chips), z)[kind]
        return remote(
            place,
            place,
            tok_send.at[0],
            tok_recv.at[2 * slot + part],
            x,
            y,
            to_z,
            1 - c if kind == 2 else c,
        )

    def part_copy(k, owner):
        return pltpu.make_async_remote_copy(
            src_ref=mod_parts.at[owner],
            dst_ref=mod_parts.at[owner],
            send_sem=part_sem.at[0],
            recv_sem=part_sem.at[1],
            device_id={"sp": lax.rem(s + k, sp_size), "tp": t},
            device_id_type=MESH,
        )

    def piece_copy(k, owner):
        return pltpu.make_async_remote_copy(
            src_ref=mod_pieces.at[owner],
            dst_ref=mod_pieces.at[owner],
            send_sem=piece_sem.at[0],
            recv_sem=piece_sem.at[1],
            device_id={"sp": s, "tp": lax.rem(t + k, tp_size)},
            device_id_type=MESH,
        )

    for k in range(1, sp_size):
        part_copy(k, s).start()
    token_copy(0, z, c, 0).start()
    token_copy(1, z, c, 1).start()
    for part in range(2):
        token_copy(2, z, c, part).start()

    awaited(mod_parts.at[0 : sp_size - 1], part_sem.at[1])
    total = mod_parts[0]
    for i in range(1, sp_size):
        total = total + mod_parts[i]
    mod_pieces[t] = total
    mod_pieces[t, 6:7, :] = jnp.full((1, piece), lambdas[0], jnp.float32)
    mod_pieces[t, 7:8, :] = jnp.full((1, piece), lift[0], jnp.float32)
    for k in sorted(range(1, tp_size), key=lambda k: -min(k, tp_size - k)):
        piece_copy(k, t).start()
    token_copy(0, z, c, 1).start()
    token_copy(1, z, c, 0).start()

    def forward(d, early):
        left = ring(z - d, chips)
        right = ring(z + d, chips)
        right_part, left_part = (0, 1) if early else (1, 0)
        token_copy(2, left, c, right_part).wait_recv()
        if d + 1 < far or (d + 1 == far and early):
            token_copy(0, left, c, right_part).start()
        token_copy(2, left, c, right_part).start()
        token_copy(2, right, c, left_part).wait_recv()
        if d + 1 < far or (d + 1 == far and early):
            token_copy(1, right, c, left_part).start()
        token_copy(2, right, c, left_part).start()

    forward(1, True)
    awaited(mod_pieces.at[0 : tp_size - 1], piece_sem.at[1])
    for i in range(tp_size):
        mod_rows[:, i * piece : (i + 1) * piece] = mod_pieces[i]

    def normalise(source, base, dest, count, row):
        v = source[aligned(base, count), :].astype(jnp.float32)
        v = v - jnp.sum(v, axis=1, keepdims=True) * (1.0 / width)
        spread = jnp.sum(v * v, axis=1, keepdims=True) * (1.0 / width)
        v = v * lax.rsqrt(spread + EPSILON)
        v = v * (1.0 + mod_rows[2 + row : 3 + row, :]) + mod_rows[row : row + 1, :]
        normed[aligned(dest, count), :] = v.astype(jnp.bfloat16)

    sizes = (ctx_rows + pair, 2 * pair, 2 * pair, 2 * pair, pair)
    starts = tuple(sum(sizes[:g]) for g in range(GROUPS))
    firsts = (pair, pair, pair, pair, 3 * pair // 4)
    halves = tuple((firsts[g], sizes[g] - firsts[g]) for g in range(GROUPS))
    transit_starts = tuple(SIDE * sum(h[1] for h in halves[:g]) for g in range(GROUPS))
    own_kind = p == c
    other_kind = p != c
    xs = [x, lax.rem(x + 1, SIDE), lax.rem(x + 2, SIDE), lax.rem(x + 3, SIDE)]
    ys = [y, lax.rem(y + 1, SIDE), lax.rem(y + 2, SIDE), lax.rem(y + 3, SIDE)]

    def kv_at(g, q, sx, sy, count=1):
        n = halves[g][q]
        order = sx * SIDE + sy if q else sy * SIDE + sx
        start = sp_size * (starts[g] + q * halves[g][0])
        return keys_values.at[aligned(start + order * n, count * n)]

    def transit_at(g, sy, count=1):
        n = halves[g][1]
        return transit.at[aligned(transit_starts[g] + sy * n, count * n)]

    def stage_at(g, q):
        return stage.at[aligned(starts[g] + q * halves[g][0], halves[g][q])]

    def send(step, src, dst, recv_sem, sx, sy, sc):
        return remote(src, dst, kv_send.at[min(step - 1, 2)], recv_sem, sx, sy, z, sc)

    def handed_at(g):
        return handed.at[aligned(sum(h[0] for h in halves[:g]), halves[g][0])]

    def leaving(g, step, core=None):
        mine = []
        here = stage_at(g, core) if step == 1 else None

        def add(cond, *args):
            mine.append((cond, send(step, *args)))

        def on(ref):
            add(None, ref, ref, dd_all.at[g], x, y, 1 - c)

        def along_row(straight, aside, own, other):
            there = kv_at(g, 0, x, y)
            sem = stage_recv.at[g, 0]
            add(other, aside, there, sem, xs[1], y, 0)
            add(other, aside, there, sem, xs[3], y, 0)
            add(own, straight, there, sem, xs[2], y, 0)

        def along_column(straight, aside, own, other):
            for cond, ref, there in ((own, straight, kv_at(g, 1, x, y)), (other, aside, transit_at(g, y))):
                for k in (1, 3):
                    add(cond, ref, there, stage_recv.at[g, 0], x, ys[k], 1)

        if step == 1:
            there = kv_at(g, 1 - core, x, y)
            far_half = stage_at(g, 1 - core)
            add(own_kind, far_half, there, dd_own.at[g], x, y, 1 - c)
            add(other_kind, far_half, handed_at(g) if core else transit_at(g, y), dd_own.at[g], x, y, 1 - c)
            (along_column if core else along_row)(here, here, own_kind, other_kind)
            add(own_kind, here, kv_at(g, core, x, y), dd_ownb.at[g], x, y, 1 - c)
        elif core == 0:
            if step == 2:
                along_row(kv_at(g, 0, x, y), handed_at(g), other_kind, own_kind)
            if step == 3:
                line = kv_at(g, 0, 0, y, SIDE)
                add(None, line, line, stage_recv.at[g, 1], x, ys[1], 0)
                add(None, line, line, stage_recv.at[g, 1], x, ys[3], 0)
                for k in (1, 2, 3):
                    on(kv_at(g, 0, xs[k], y))
            if step == 4:
                low = kv_at(g, 0, 0, ys[3], 2)
                high = kv_at(g, 0, 2, ys[1], 2)
                add(None, low, low, stage_recv.at[g, 2], x, ys[1], 0)
                add(None, high, high, stage_recv.at[g, 2], x, ys[3], 0)
                on(kv_at(g, 0, 0, ys[3], SIDE))
                on(kv_at(g, 0, 0, ys[1], SIDE))
            if step == 5:
                on(kv_at(g, 0, 0, ys[2], SIDE))
        else:
            if step == 2:
                along_column(kv_at(g, 1, x, y), transit_at(g, y), other_kind, own_kind)
            if step == 3:
                below = kv_at(g, 1, x, ys[3])
                above = transit_at(g, ys[1])
                add(None, below, below, stage_recv.at[g, 1], x, ys[1], 1)
                add(None, above, above, stage_recv.at[g, 1], x, ys[3], 1)
                on(below)
                on(kv_at(g, 1, x, ys[1]))
            if step == 4:
                line = kv_at(g, 1, x, 0, SIDE)
                passing = transit_at(g, 0, SIDE)
                add(None, line, line, stage_recv.at[g, 2], xs[2], y, 1)
                add(None, passing, line, stage_recv.at[g, 2], xs[1], y, 1)
                add(None, passing, line, stage_recv.at[g, 2], xs[3], y, 1)
                on(kv_at(g, 1, x, ys[2]))
            if step == 5:
                for k in (1, 2, 3):
                    on(kv_at(g, 1, xs[k], 0, SIDE))
        return mine

    def arriving(g, step, core):
        n = halves[g][core]
        if step == 2:
            awaited(keys_values.at[0:n], dd_own.at[g])
        else:
            blocks = ((3, 8, 4), (4, 2, 12))[core][step - 3]
            awaited(keys_values.at[0 : blocks * n], stage_recv.at[g, step - 3])

    def go(copies, wait=False):
        for cond, copy in copies:
            act = copy.wait_send if wait else copy.start
            if cond is None:
                act()
            else:
                pl.when(cond)(act)

    def relay(core, *stages):
        @pl.when(c == core)
        def _():
            for g, step in stages:
                arriving(g, step, core)
                go(leaving(g, step, core))

    def complete(g):
        for core in range(2):

            @pl.when(c == core)
            def _():
                n = halves[g][1 - core]
                awaited(keys_values.at[0 : 15 * n], dd_all.at[g])

                @pl.when(other_kind)
                def _():
                    awaited(keys_values.at[0:n], dd_ownb.at[g])

    def hand_out(g, keys, values):
        stage[starts[g] : starts[g] + sizes[g], :head] = keys
        stage[starts[g] : starts[g] + sizes[g], head:] = values
        for core in range(2):
            pl.when(c == core)(functools.partial(go, leaving(g, 1, core)))
        parts = (slice(0, halves[g][0]), slice(halves[g][0], sizes[g]))

        @pl.when(own_kind)
        def _():
            for q in range(2):
                place = kv_at(g, q, x, y)
                place[:, :head] = keys[parts[q]]
                place[:, head:] = values[parts[q]]

        @pl.when(other_kind & (c == 1))
        def _():
            place = transit_at(g, y)
            place[:, :head] = keys[parts[1]]
            place[:, head:] = values[parts[1]]

    q_parts = ((0, 5 * pair), (5 * pair, 3 * pair))

    def q_copy(i):
        place = aligned(*q_parts[i])
        return remote(
            q_stage.at[place],
            queries.at[place],
            q_sem.at[2],
            q_sem.at[i],
            x + 1 - 2 * p,
            y,
            z,
            1 - c,
        )

    quarter = half // 4
    lane = lax.broadcasted_iota(jnp.int32, (pair, half), 1)
    by_row = lane < half // 2
    low = lax.rem(lax.broadcasted_iota(jnp.int32, (1, half), 1), 2 * quarter) < quarter
    factor = half ** (-0.5) * LOG2E

    def angles(blocks):
        found = []
        for row_table, col_table in ((row_cos, col_cos), (row_sin, col_sin)):
            found.append(
                jnp.concatenate(
                    [
                        jnp.where(by_row, row_table[pl.ds(s * chips + b, 1), :], col_table[...])
                        for b in blocks
                    ],
                    axis=0,
                )
            )
        return found

    def turn(raw, cos, sin, scale=None):
        parts = []
        for i in range(head // half):
            v = raw[:, i * half : (i + 1) * half].astype(jnp.bfloat16).astype(jnp.float32)
            other = jnp.where(low, pltpu.roll(v, half - quarter, 1), pltpu.roll(v, quarter, 1))
            turned = v * cos + other * sin
            if scale is not None:
                turned = turned * scale
            parts.append(turned.astype(jnp.bfloat16))
        return jnp.concatenate(parts, axis=1)

    def from_partner(b):
        for part in range(2):
            token_copy(2, b, 1 - c, part).wait_recv()

    def ask(i, blocks):
        first_row, n = q_parts[i]
        at = slice(first_row, first_row + n)
        cos, sin = angles(blocks)
        found = jnp.dot(
            normed[ctx_rows + first_row : ctx_rows + first_row + n, :],
            wq[...],
            preferred_element_type=jnp.float32,
        )
        found = turn(found, cos, sin, factor)

        @pl.when(own_kind)
        def _():
            queries[at, :] = found

        @pl.when(other_kind)
        def _():
            q_stage[at, :] = found
            q_copy(i).start()

    from_partner(z)
    locals_[2].wait()
    normalise(context_tokens, 0, 0, ctx_rows, 1)
    normalise(tokens, z * pair, ctx_rows, pair, 0)
    for i in (3, 4, 5):
        locals_[i].wait()
    cos, sin = angles([z])
    found = jnp.dot(normed[: sizes[0], :], wk[...], preferred_element_type=jnp.float32)
    keys = jnp.concatenate([found[:ctx_rows].astype(jnp.bfloat16), turn(found[ctx_rows:], cos, sin)], axis=0)
    values = jnp.dot(normed[: sizes[0], :], wv[...], preferred_element_type=jnp.float32).astype(jnp.bfloat16)
    hand_out(0, keys, values)
    forward(1, False)

    def process(d, carry):
        left = ring(z - d, chips)
        right = ring(z + d, chips)

        @pl.when(d == 2)
        def _():
            relay(0, (0, 3))
            relay(1, (0, 3))

        from_partner(left)
        from_partner(right)
        base = starts[1] + (d - 1) * 2 * pair
        normalise(tokens, left * pair, base, pair, 0)
        normalise(tokens, right * pair, base + pair, pair, 0)

        @pl.when(d == 1)
        def _():
            forward(2, True)
            relay(0, (0, 2))
            relay(1, (0, 2))

        @pl.when(d == 2)
        def _():
            forward(3, True)

        @pl.when(d == 3)
        def _():
            opposite = ring(z + far, chips)
            token_copy(2, opposite, c, 0).wait_recv()
            token_copy(2, opposite, c, 0).start()
            relay(0, (0, 4))
            relay(1, (1, 4))

        cos, sin = angles([left, right])
        v = normed[aligned(base, 2 * pair), :]
        keys = turn(jnp.dot(v, wk[...], preferred_element_type=jnp.float32), cos, sin)
        values = jnp.dot(v, wv[...], preferred_element_type=jnp.float32).astype(jnp.bfloat16)
        for g in (1, 2, 3):
            pl.when(d == g)(functools.partial(hand_out, g, keys, values))

        @pl.when(d == 1)
        def _():
            forward(2, False)
            relay(0, (1, 2))
            relay(1, (1, 2))

        @pl.when(d == 3)
        def _():
            relay(1, (2, 3))

        @pl.when(d == 2)
        def _():
            relay(0, (1, 3))
            relay(1, (1, 3), (0, 4))
            around = [z]
            for k in (1, 2):
                around += [ring(z - k, chips), ring(z + k, chips)]
            ask(0, around)
            relay(0, (2, 2))
            relay(1, (2, 2))
            forward(3, False)

        return carry

    lax.fori_loop(1, 4, process, 0)

    opposite = ring(z + far, chips)
    token_copy(2, opposite, c, 1).wait_recv()
    token_copy(2, opposite, c, 1).start()
    relay(0, (3, 2))
    relay(1, (3, 2))
    from_partner(opposite)
    normalise(tokens, opposite * pair, starts[4], pair, 0)
    relay(0, (1, 4))
    relay(1, (0, 5))
    cos, sin = angles([opposite])
    v = normed[starts[4] : starts[4] + pair, :]
    keys = turn(jnp.dot(v, wk[...], preferred_element_type=jnp.float32), cos, sin)
    values = jnp.dot(v, wv[...], preferred_element_type=jnp.float32).astype(jnp.bfloat16)
    hand_out(4, keys, values)
    relay(0, (2, 3))
    ask(1, [ring(z - 3, chips), ring(z + 3, chips), opposite])
    relay(0, (4, 2), (0, 5))
    relay(1, (2, 4), (4, 2), (3, 3))

    peak[...] = jnp.full(peak.shape, -jnp.inf, jnp.float32)
    total_weight[...] = jnp.zeros(total_weight.shape, jnp.float32)
    mixed[...] = jnp.zeros(mixed.shape, jnp.float32)

    def await_queries(i):
        @pl.when(other_kind)
        def _():
            awaited(queries.at[aligned(*q_parts[i])], q_sem.at[i])

    my_head = 2 * z + p
    weight_of_second = mod_pieces[my_head, 6:7, 0:1]
    lifted = mod_pieces[my_head, 7:8, 0:1] * LOG2E

    def attend(base, count, first_row, n, raised=None):
        keys_at = aligned(base, count)
        at = aligned(first_row, n)
        scores = [
            lax.dot_general(
                queries[at, m * half : (m + 1) * half],
                keys_values[keys_at, m * half : (m + 1) * half],
                (((1,), (1,)), ((), ())),
                preferred_element_type=jnp.float32,
            )
            for m in range(2)
        ]
        for m in range(2):
            score = scores[m] if raised is None else scores[m] + raised
            old = peak[m, at, :]
            new = jnp.maximum(old, jnp.max(score, axis=1, keepdims=True))
            alpha = jnp.exp2(old - new)
            weights = jnp.exp2(score - new[:, :1])
            total_weight[m, at, :] = total_weight[m, at, :] * alpha + jnp.sum(
                weights, axis=1, keepdims=True
            )
            peak[m, at, :] = new
            mixed[m, at, :] = mixed[m, at, :] * alpha[:, :1] + jnp.dot(
                weights.astype(jnp.bfloat16),
                keys_values[keys_at, head:],
                preferred_element_type=jnp.float32,
            )

    def out_copy(i, first_row, n):
        return remote(
            out_stage.at[first_row : first_row + n],
            attended.at[first_row : first_row + n],
            out_sem.at[3],
            out_sem.at[i],
            x + 1 - 2 * p,
            y,
            z,
            1 - c,
        )

    tiles = ((7 * pair, pair), (5 * pair, 2 * pair), q_parts[0])

    def finish(i):
        first_row, n = tiles[i]
        at = slice(first_row, first_row + n)
        diff = mixed[0, at, :] / total_weight[0, at, :1] - weight_of_second * (
            mixed[1, at, :] / total_weight[1, at, :1]
        )
        mean = jnp.sum(diff * diff, axis=1, keepdims=True) * (1.0 / head)
        found = (diff * lax.rsqrt(mean + EPSILON) * gain[...]).astype(jnp.bfloat16)

        @pl.when(own_kind)
        def _():
            attended[at, :] = found

        @pl.when(other_kind)
        def _():
            out_stage[at, :] = found
            out_copy(i, first_row, n).start()

    count = sp_size * sizes[0]
    column = lax.broadcasted_iota(jnp.int32, (1, count), 1)
    on_context = (column < sp_size * halves[0][0]) & (lax.rem(column, halves[0][0]) < ctx_rows)
    raised = jnp.where(on_context, lifted, 0.0)
    tile = block_tokens // 2

    await_queries(0)
    complete(0)

    def first_group(i, carry):
        attend(0, count, i * tile, tile, raised)

        @pl.when(i == 0)
        def _():
            await_queries(1)
            relay(0, (1, 5))
            relay(1, (1, 5), (4, 3))

        return carry

    lax.fori_loop(0, 2, first_group, 0)
    relay(0, (2, 4), (3, 3))
    relay(1, (3, 4))
    complete(1)

    def groups(j, carry):
        g = lax.div(j, 2) + 1
        i = lax.rem(j, 2)
        attend(sp_size * (starts[1] + (g - 1) * sizes[1]), sp_size * sizes[1], i * tile, tile)

        @pl.when(j == 0)
        def _():
            relay(0, (4, 3))
            relay(1, (4, 4))

        @pl.when(j == 1)
        def _():
            relay(0, (2, 5))
            relay(1, (2, 5))
            complete(2)

        @pl.when(j == 2)
        def _():
            relay(0, (3, 4))
            relay(1, (3, 5))

        return carry

    lax.fori_loop(0, 4, groups, 0)
    relay(0, (4, 4), (3, 5))
    complete(3)
    locals_[6].wait()
    base = sp_size * starts[3]
    count = sp_size * sizes[3]
    rest = sp_size * sizes[4]
    attend(base, count, *q_parts[1])
    relay(0, (4, 5))
    relay(1, (4, 5))
    complete(4)
    for i in range(2):
        attend(base + count, rest, *tiles[i])
        finish(i)
    attend(base, count, *tiles[2])

    span = width // 2
    chunk = 1024

    def pair_copy(u):
        ref = pair_send.at[u]
        return remote(ref, pair_recv.at[u], ps_sem.at[0], pr_sem.at[u], x, y, z, 1 - c)

    def ring_copy(side, d, part):
        u = 2 * d + part
        into = (from_left, from_right)[side]
        sem = (left_sem, right_sem)[side]
        to = (ring(z + 1, chips), ring(z - 1, chips))[side]
        v = 2 * (d - 1) + part
        return remote(
            ring_stage.at[side, u], into.at[v], st_sem.at[side], sem.at[v], x, y, to, c
        )

    def ring_arrived(side, d, part):
        v = 2 * d + part
        into = (from_left, from_right)[side]
        sem = (left_sem, right_sem)[side]
        awaited(into.at[v], sem.at[v])

    def block_of(side, d):
        if d == 0:
            return 0
        if d == far:
            return 2 * far - 1
        return 2 * d if side == 0 else 2 * d - 1

    def compute(d):
        blocks = [block_of(0, d)] if d in (0, far) else [block_of(1, d), block_of(0, d)]
        others = [attended[aligned(j * pair + (1 - c) * rows, rows), :] for j in blocks]
        mines = [attended[aligned(j * pair + c * rows, rows), :] for j in blocks]
        both = jnp.concatenate(others + mines, axis=0)
        n = len(blocks)
        for part in range(2):
            for k in range(span // chunk):
                found = jnp.dot(
                    both,
                    wo[:, part * span + k * chunk : part * span + (k + 1) * chunk],
                    preferred_element_type=jnp.float32,
                )
                cols = slice(k * chunk, (k + 1) * chunk)
                for i, j in enumerate(blocks):
                    pair_send[2 * j + part, :, cols] = found[i * rows : (i + 1) * rows].astype(jnp.bfloat16)
                    own[2 * j + part, :, cols] = found[(n + i) * rows : (n + i + 1) * rows]
            for j in blocks:
                pair_copy(2 * j + part).start()

    def combine(side, d, part):
        u = 2 * block_of(side, d) + part
        pair_copy(u).wait_recv()
        value = own[u] + pair_recv[u].astype(jnp.float32)
        if not (d == far or (d == far - 1 and part != side)):
            ring_arrived(side, d, part)
            value = value + (from_left, from_right)[side][2 * d + part].astype(jnp.float32)
        ring_stage[side, 2 * d + part] = value.astype(jnp.bfloat16)
        ring_copy(side, d, part).start()

    def await_attended(i):
        @pl.when(other_kind)
        def _():
            awaited(attended.at[aligned(*tiles[i])], out_sem.at[i])

    await_attended(0)
    compute(4)
    combine(0, 4, 0)
    combine(1, 4, 1)
    await_attended(1)
    compute(3)
    combine(0, 3, 1)
    combine(1, 3, 0)
    attend(base + count, rest, *tiles[2])
    finish(2)
    combine(0, 3, 0)
    combine(1, 3, 1)

    await_attended(2)
    compute(2)
    combine(0, 2, 1)
    combine(1, 2, 0)
    compute(1)

    awaited(tokens.at[0 : 2 * (2 * far - 1) * part_rows + block_tokens // 2], tok_send.at[0])
    awaited(mod_parts.at[0 : sp_size - 1], part_sem.at[0])
    awaited(mod_pieces.at[0 : tp_size - 1], piece_sem.at[0])
    combine(0, 2, 0)
    combine(1, 2, 1)
    compute(0)
    first_rows = sum(h[0] for h in halves)
    second_rows = sum(h[1] for h in halves)
    for core in range(2):
        for cond, kind in ((own_kind, 0), (other_kind, 1)):

            @pl.when((c == core) & cond)
            def _():
                alone = (first_rows, second_rows)[core]
                away = (first_rows, second_rows)[1 - core]
                own_sends, later = ((2, 27), (3, 29))[core]
                once = away + (own_sends if kind == 0 else 2) * alone
                handed_on = (1 if core == 0 and kind == 1 else 2) * alone
                awaited(keys_values.at[0:once], kv_send.at[0])
                awaited(keys_values.at[0:handed_on], kv_send.at[1])
                awaited(keys_values.at[0 : later * alone], kv_send.at[2])

    @pl.when(other_kind)
    def _():
        awaited(queries, q_sem.at[2])
        awaited(attended, out_sem.at[3])

    awaited(pair_send, ps_sem.at[0])
    combine(0, 1, 1)
    combine(1, 1, 0)
    combine(0, 1, 0)
    combine(1, 1, 1)

    for part in (1, 0):
        cols = slice(part * span, (part + 1) * span)
        pair_copy(part).wait_recv()
        value = own[part] + pair_recv[part].astype(jnp.float32)
        ring_arrived(0, 0, part)
        value = value + from_left[part].astype(jnp.float32)
        ring_arrived(1, 0, part)
        value = value + from_right[part].astype(jnp.float32)
        result[:, cols] = (
            tokens[aligned(t * rows, rows), cols].astype(jnp.float32) + mod_rows[4:5, cols] * value
        ).astype(jnp.bfloat16)

    for side in range(2):
        awaited(ring_stage.at[side, 0 : 2 * far - 1], st_sem.at[side])


def tables(half):
    quarter = half // 4
    inverse = (ROPE_BASE ** (-np.arange(quarter, dtype=np.float32) / quarter)).astype(np.float32)
    inverse = np.tile(inverse, 4)
    sign = np.where(np.arange(half) % (2 * quarter) < quarter, -1.0, 1.0).astype(np.float32)
    found = []
    for count in (8192 // GRID_W, GRID_W):
        angle = np.arange(count, dtype=np.float32)[:, None] * inverse[None, :]
        found.append(np.cos(angle).astype(np.float32))
        found.append((np.sin(angle) * sign).astype(np.float32))
    return found


def shards(
    sp_size,
    tp_size,
    latent,
    context,
    condition,
    context_condition,
    modulation,
    query_weight,
    key_weight,
    value_weight,
    lambdas,
    context_lift,
    head_gain,
    output_weight,
):
    rows, width = latent.shape
    chips = tp_size // 2
    head = query_weight.shape[1]
    half = head // 2
    pair = 2 * rows
    block_tokens = rows * tp_size
    ctx_rows = context.shape[0]
    piece = modulation.shape[2]
    vmem = pl.BlockSpec(memory_space=pltpu.VMEM)
    smem = pl.BlockSpec(memory_space=pltpu.SMEM)
    anywhere = pl.BlockSpec(memory_space=pl.ANY)
    bf16, f32 = jnp.bfloat16, jnp.float32
    dma = pltpu.SemaphoreType.DMA
    blocks = (2 * chips, rows, width // 2)
    row_cos, row_sin, col_cos, col_sin = tables(half)
    return pl.pallas_call(
        functools.partial(kernel, sp_size, tp_size),
        out_shape=jax.ShapeDtypeStruct((rows, width), bf16),
        in_specs=[anywhere] * 2 + [vmem] * 2 + [anywhere] * 4 + [vmem] * 4 + [smem] * 2 + [vmem, anywhere],
        out_specs=vmem,
        scratch_shapes=[
            pltpu.VMEM((block_tokens, width), bf16),
            pltpu.VMEM(context.shape, bf16),
            pltpu.VMEM((ctx_rows + block_tokens, width), bf16),
            pltpu.VMEM(modulation.shape, bf16),
            pltpu.VMEM((width, head), bf16),
            pltpu.VMEM((width, head), bf16),
            pltpu.VMEM((width, head), bf16),
            pltpu.VMEM((head, width), bf16),
            pltpu.VMEM((sp_size * (ctx_rows + block_tokens), 2 * head), bf16),
            pltpu.VMEM((SIDE * block_tokens // 2, 2 * head), bf16),
            pltpu.VMEM((ctx_rows + block_tokens, 2 * head), bf16),
            pltpu.VMEM((block_tokens, head), bf16),
            pltpu.VMEM((block_tokens, head), bf16),
            pltpu.VMEM((2, block_tokens, 128), f32),
            pltpu.VMEM((2, block_tokens, 128), f32),
            pltpu.VMEM((2, block_tokens, head), f32),
            pltpu.VMEM((block_tokens, head), bf16),
            pltpu.VMEM((block_tokens, head), bf16),
            pltpu.VMEM((sp_size, 8, piece), f32),
            pltpu.VMEM((tp_size, 8, piece), f32),
            pltpu.VMEM((8, width), f32),
            pltpu.VMEM(blocks, f32),
            pltpu.VMEM(blocks, bf16),
            pltpu.VMEM(blocks, bf16),
            pltpu.VMEM((2, chips + 2, rows, width // 2), bf16),
            pltpu.VMEM((chips, rows, width // 2), bf16),
            pltpu.VMEM((chips, rows, width // 2), bf16),
            pltpu.VMEM((5 * pair, 2 * head), bf16),
            dma((7,)),
            dma((1,)),
            dma((2 * tp_size,)),
            dma((2,)),
            dma((2,)),
            dma((3,)),
            dma((5, 3)),
            dma((5,)),
            dma((5,)),
            dma((5,)),
            dma((3,)),
            dma((4,)),
            dma((1,)),
            dma((2 * chips,)),
            dma((2,)),
            dma((chips,)),
            dma((chips,)),
        ],
        compiler_params=pltpu.CompilerParams(
            collective_id=0, has_side_effects=True, vmem_limit_bytes=VMEM_LIMIT
        ),
        name="layer",
    )(
        latent,
        context,
        condition.reshape(1, -1),
        context_condition.reshape(1, -1),
        modulation,
        query_weight,
        key_weight,
        value_weight,
        jnp.asarray(row_cos),
        jnp.asarray(row_sin),
        jnp.asarray(col_cos),
        jnp.asarray(col_sin),
        lambdas,
        context_lift,
        head_gain.reshape(1, -1),
        output_weight,
    )


def solution(mesh):
    in_specs = (
        P(("sp", "tp"), None),
        P("sp", None),
        P(),
        P(),
        P(None, "sp", "tp"),
        P(None, "tp"),
        P(None, "tp"),
        P(None, "tp"),
        P("tp"),
        P("tp"),
        P(),
        P("tp", None),
    )
    out_specs = P(("sp", "tp"), None)
    body = functools.partial(shards, mesh.shape["sp"], mesh.shape["tp"])
    return jax.shard_map(body, mesh=mesh, in_specs=in_specs, out_specs=out_specs, check_vma=False)
```

```python
import functools

import jax
import jax.numpy as jnp
import numpy as np
from jax import lax
from jax.experimental import pallas as pl
from jax.experimental.pallas import tpu as pltpu
from jax.sharding import PartitionSpec as P

GRID_W = 64
ROPE_BASE = 10000.0
EPSILON = 1e-05
LOG2E = 1.4426950408889634
ROWS = 16
SIDE = 4
VMEM_LIMIT = 63 * 1024 * 1024
MESH = pl.DeviceIdType.MESH
GROUPS = 5


def aligned(start, size, unit=ROWS):
    return pl.ds(pl.multiple_of(start, unit), size)


def kernel(
    sp_size,
    tp_size,
    latent,
    context,
    condition,
    context_condition,
    modulation,
    query_weight,
    key_weight,
    value_weight,
    row_cos,
    row_sin,
    col_cos,
    col_sin,
    lambdas,
    lift,
    gain,
    output_weight,
    result,
    tokens,
    context_tokens,
    normed,
    mod_weight,
    wq,
    wk,
    wv,
    wo,
    keys_values,
    transit,
    stage,
    queries,
    q_stage,
    peak,
    total_weight,
    mixed,
    attended,
    out_stage,
    mod_parts,
    mod_pieces,
    mod_rows,
    own,
    pair_send,
    pair_recv,
    ring_stage,
    from_left,
    from_right,
    handed,
    local_sem,
    tok_send,
    tok_recv,
    part_sem,
    piece_sem,
    kv_send,
    stage_recv,
    dd_own,
    dd_ownb,
    dd_all,
    q_sem,
    out_sem,
    ps_sem,
    pr_sem,
    st_sem,
    left_sem,
    right_sem,
):
    s = lax.axis_index("sp")
    t = lax.axis_index("tp")
    y = lax.div(s, SIDE)
    x = lax.rem(s, SIDE)
    z = lax.div(t, 2)
    c = lax.rem(t, 2)
    p = lax.rem(x, 2)
    chips = tp_size // 2
    far = chips // 2
    rows, width = latent.shape
    pair = 2 * rows
    block_tokens = tp_size * rows
    ctx_rows = context.shape[0]
    head = query_weight.shape[1]
    half = head // 2
    piece = modulation.shape[2]
    depth = modulation.shape[1]

    def ring(v, n):
        return lax.rem(v + n, n)

    def awaited(ref, sem):
        pltpu.make_async_copy(ref, ref, sem).wait()

    def remote(src, dst, send_sem, recv_sem, sx, sy, sz, sc):
        return pltpu.make_async_remote_copy(
            src_ref=src,
            dst_ref=dst,
            send_sem=send_sem,
            recv_sem=recv_sem,
            device_id={"sp": sy * SIDE + sx, "tp": 2 * sz + sc},
            device_id_type=MESH,
        )

    own_slot = tokens.at[aligned(t * rows, rows)]
    locals_ = [
        pltpu.make_async_copy(src, dst, local_sem.at[i])
        for i, (src, dst) in enumerate(
            [
                (modulation, mod_weight),
                (latent, own_slot),
                (context, context_tokens),
                (key_weight, wk),
                (value_weight, wv),
                (query_weight, wq),
                (output_weight, wo),
            ]
        )
    ]
    for copy in locals_:
        copy.start()

    barrier = pltpu.get_barrier_semaphore()
    for k in range(1, tp_size):
        pl.semaphore_signal(
            barrier, inc=1, device_id={"sp": s, "tp": lax.rem(t + k, tp_size)}, device_id_type=MESH
        )
    for k in range(1, sp_size):
        pl.semaphore_signal(
            barrier, inc=1, device_id={"sp": lax.rem(s + k, sp_size), "tp": t}, device_id_type=MESH
        )
    near = [(1, 0), (2, 0), (3, 0), (0, 1), (0, 3)]
    for dx, dy in near:
        pl.semaphore_signal(
            barrier,
            inc=1,
            device_id={
                "sp": lax.rem(y + dy, SIDE) * SIDE + lax.rem(x + dx, SIDE),
                "tp": 2 * z + 1 - c,
            },
            device_id_type=MESH,
        )

    def silu(ref):
        v = ref[:, aligned(s * depth, depth, 128)]
        return v / (1.0 + jnp.exp(-v))

    first = silu(condition)
    second = silu(context_condition)
    which = lax.broadcasted_iota(jnp.int32, (ROWS, depth), 0)
    vectors = jnp.where(
        which == 0, jnp.broadcast_to(first, (ROWS, depth)), jnp.broadcast_to(second, (ROWS, depth))
    ).astype(jnp.bfloat16)
    locals_[0].wait()
    for r in range(3):
        found = jnp.dot(vectors, mod_weight[r], preferred_element_type=jnp.float32)
        mod_parts[s, 2 * r : 2 * r + 2, :] = found[0:2]
    mod_parts[s, 6:8, :] = jnp.zeros((2, piece), jnp.float32)
    locals_[1].wait()

    pl.semaphore_wait(barrier, tp_size + sp_size - 2 + len(near))

    part_rows = rows // 2

    def token_copy(kind, b, core, part):
        slot = 2 * b + core
        place = tokens.at[aligned(slot * rows + part * part_rows, part_rows)]
        to_z = (ring(z + 1, chips), ring(z - 1, chips), z)[kind]
        return remote(
            place,
            place,
            tok_send.at[0],
            tok_recv.at[2 * slot + part],
            x,
            y,
            to_z,
            1 - c if kind == 2 else c,
        )

    def part_copy(k, owner):
        return pltpu.make_async_remote_copy(
            src_ref=mod_parts.at[owner],
            dst_ref=mod_parts.at[owner],
            send_sem=part_sem.at[0],
            recv_sem=part_sem.at[1],
            device_id={"sp": lax.rem(s + k, sp_size), "tp": t},
            device_id_type=MESH,
        )

    def piece_copy(k, owner):
        return pltpu.make_async_remote_copy(
            src_ref=mod_pieces.at[owner],
            dst_ref=mod_pieces.at[owner],
            send_sem=piece_sem.at[0],
            recv_sem=piece_sem.at[1],
            device_id={"sp": s, "tp": lax.rem(t + k, tp_size)},
            device_id_type=MESH,
        )

    for k in range(1, sp_size):
        part_copy(k, s).start()
    token_copy(0, z, c, 0).start()
    token_copy(1, z, c, 1).start()
    for part in range(2):
        token_copy(2, z, c, part).start()

    awaited(mod_parts.at[0 : sp_size - 1], part_sem.at[1])
    total = mod_parts[0]
    for i in range(1, sp_size):
        total = total + mod_parts[i]
    mod_pieces[t] = total
    mod_pieces[t, 6:7, :] = jnp.full((1, piece), lambdas[0], jnp.float32)
    mod_pieces[t, 7:8, :] = jnp.full((1, piece), lift[0], jnp.float32)
    for k in sorted(range(1, tp_size), key=lambda k: -min(k, tp_size - k)):
        piece_copy(k, t).start()
    token_copy(0, z, c, 1).start()
    token_copy(1, z, c, 0).start()

    def forward(d, early):
        left = ring(z - d, chips)
        right = ring(z + d, chips)
        right_part, left_part = (0, 1) if early else (1, 0)
        token_copy(2, left, c, right_part).wait_recv()
        if d + 1 < far or (d + 1 == far and early):
            token_copy(0, left, c, right_part).start()
        token_copy(2, left, c, right_part).start()
        token_copy(2, right, c, left_part).wait_recv()
        if d + 1 < far or (d + 1 == far and early):
            token_copy(1, right, c, left_part).start()
        token_copy(2, right, c, left_part).start()

    forward(1, True)
    awaited(mod_pieces.at[0 : tp_size - 1], piece_sem.at[1])
    for i in range(tp_size):
        mod_rows[:, i * piece : (i + 1) * piece] = mod_pieces[i]

    def normalise(source, base, dest, count, row):
        v = source[aligned(base, count), :].astype(jnp.float32)
        v = v - jnp.sum(v, axis=1, keepdims=True) * (1.0 / width)
        spread = jnp.sum(v * v, axis=1, keepdims=True) * (1.0 / width)
        v = v * lax.rsqrt(spread + EPSILON)
        v = v * (1.0 + mod_rows[2 + row : 3 + row, :]) + mod_rows[row : row + 1, :]
        normed[aligned(dest, count), :] = v.astype(jnp.bfloat16)

    sizes = (ctx_rows + pair, 2 * pair, 2 * pair, 2 * pair, pair)
    starts = tuple(sum(sizes[:g]) for g in range(GROUPS))
    firsts = (pair, pair, pair, pair, 3 * pair // 4)
    halves = tuple((firsts[g], sizes[g] - firsts[g]) for g in range(GROUPS))
    transit_starts = tuple(SIDE * sum(h[1] for h in halves[:g]) for g in range(GROUPS))
    own_kind = p == c
    other_kind = p != c
    xs = [x, lax.rem(x + 1, SIDE), lax.rem(x + 2, SIDE), lax.rem(x + 3, SIDE)]
    ys = [y, lax.rem(y + 1, SIDE), lax.rem(y + 2, SIDE), lax.rem(y + 3, SIDE)]

    def kv_at(g, q, sx, sy, count=1):
        n = halves[g][q]
        order = sx * SIDE + sy if q else sy * SIDE + sx
        start = sp_size * (starts[g] + q * halves[g][0])
        return keys_values.at[aligned(start + order * n, count * n)]

    def transit_at(g, sy, count=1):
        n = halves[g][1]
        return transit.at[aligned(transit_starts[g] + sy * n, count * n)]

    def stage_at(g, q):
        return stage.at[aligned(starts[g] + q * halves[g][0], halves[g][q])]

    def send(step, src, dst, recv_sem, sx, sy, sc):
        return remote(src, dst, kv_send.at[min(step - 1, 2)], recv_sem, sx, sy, z, sc)

    def handed_at(g):
        return handed.at[aligned(sum(h[0] for h in halves[:g]), halves[g][0])]

    def leaving(g, step, core=None):
        mine = []
        here = stage_at(g, core) if step == 1 else None

        def add(cond, *args):
            mine.append((cond, send(step, *args)))

        def on(ref):
            add(None, ref, ref, dd_all.at[g], x, y, 1 - c)

        def along_row(straight, aside, own, other):
            there = kv_at(g, 0, x, y)
            sem = stage_recv.at[g, 0]
            add(other, aside, there, sem, xs[1], y, 0)
            add(other, aside, there, sem, xs[3], y, 0)
            add(own, straight, there, sem, xs[2], y, 0)

        def along_column(straight, aside, own, other):
            for cond, ref, there in ((own, straight, kv_at(g, 1, x, y)), (other, aside, transit_at(g, y))):
                for k in (1, 3):
                    add(cond, ref, there, stage_recv.at[g, 0], x, ys[k], 1)

        if step == 1:
            there = kv_at(g, 1 - core, x, y)
            far_half = stage_at(g, 1 - core)
            add(own_kind, far_half, there, dd_own.at[g], x, y, 1 - c)
            add(other_kind, far_half, handed_at(g) if core else transit_at(g, y), dd_own.at[g], x, y, 1 - c)
            (along_column if core else along_row)(here, here, own_kind, other_kind)
            add(own_kind, here, kv_at(g, core, x, y), dd_ownb.at[g], x, y, 1 - c)
        elif core == 0:
            if step == 2:
                along_row(kv_at(g, 0, x, y), handed_at(g), other_kind, own_kind)
            if step == 3:
                line = kv_at(g, 0, 0, y, SIDE)
                add(None, line, line, stage_recv.at[g, 1], x, ys[1], 0)
                add(None, line, line, stage_recv.at[g, 1], x, ys[3], 0)
                for k in (1, 2, 3):
                    on(kv_at(g, 0, xs[k], y))
            if step == 4:
                low = kv_at(g, 0, 0, ys[3], 2)
                high = kv_at(g, 0, 2, ys[1], 2)
                add(None, low, low, stage_recv.at[g, 2], x, ys[1], 0)
                add(None, high, high, stage_recv.at[g, 2], x, ys[3], 0)
                on(kv_at(g, 0, 0, ys[3], SIDE))
                on(kv_at(g, 0, 0, ys[1], SIDE))
            if step == 5:
                on(kv_at(g, 0, 0, ys[2], SIDE))
        else:
            if step == 2:
                along_column(kv_at(g, 1, x, y), transit_at(g, y), other_kind, own_kind)
            if step == 3:
                below = kv_at(g, 1, x, ys[3])
                above = transit_at(g, ys[1])
                add(None, below, below, stage_recv.at[g, 1], x, ys[1], 1)
                add(None, above, above, stage_recv.at[g, 1], x, ys[3], 1)
                on(below)
                on(kv_at(g, 1, x, ys[1]))
            if step == 4:
                line = kv_at(g, 1, x, 0, SIDE)
                passing = transit_at(g, 0, SIDE)
                add(None, line, line, stage_recv.at[g, 2], xs[2], y, 1)
                add(None, passing, line, stage_recv.at[g, 2], xs[1], y, 1)
                add(None, passing, line, stage_recv.at[g, 2], xs[3], y, 1)
                on(kv_at(g, 1, x, ys[2]))
            if step == 5:
                for k in (1, 2, 3):
                    on(kv_at(g, 1, xs[k], 0, SIDE))
        return mine

    def arriving(g, step, core):
        n = halves[g][core]
        if step == 2:
            awaited(keys_values.at[0:n], dd_own.at[g])
        else:
            blocks = ((3, 8, 4), (4, 2, 12))[core][step - 3]
            awaited(keys_values.at[0 : blocks * n], stage_recv.at[g, step - 3])

    def go(copies, wait=False):
        for cond, copy in copies:
            act = copy.wait_send if wait else copy.start
            if cond is None:
                act()
            else:
                pl.when(cond)(act)

    def relay(core, *stages):
        @pl.when(c == core)
        def _():
            for g, step in stages:
                arriving(g, step, core)
                go(leaving(g, step, core))

    def complete(g):
        for core in range(2):

            @pl.when(c == core)
            def _():
                n = halves[g][1 - core]
                awaited(keys_values.at[0 : 15 * n], dd_all.at[g])

                @pl.when(other_kind)
                def _():
                    awaited(keys_values.at[0:n], dd_ownb.at[g])

    def hand_out(g, keys, values):
        stage[starts[g] : starts[g] + sizes[g], :head] = keys
        stage[starts[g] : starts[g] + sizes[g], head:] = values
        for core in range(2):
            pl.when(c == core)(functools.partial(go, leaving(g, 1, core)))
        parts = (slice(0, halves[g][0]), slice(halves[g][0], sizes[g]))

        @pl.when(own_kind)
        def _():
            for q in range(2):
                place = kv_at(g, q, x, y)
                place[:, :head] = keys[parts[q]]
                place[:, head:] = values[parts[q]]

        @pl.when(other_kind & (c == 1))
        def _():
            place = transit_at(g, y)
            place[:, :head] = keys[parts[1]]
            place[:, head:] = values[parts[1]]

    q_parts = ((0, 5 * pair), (5 * pair, 3 * pair))

    def q_copy(i):
        place = aligned(*q_parts[i])
        return remote(
            q_stage.at[place],
            queries.at[place],
            q_sem.at[2],
            q_sem.at[i],
            x + 1 - 2 * p,
            y,
            z,
            1 - c,
        )

    quarter = half // 4
    lane = lax.broadcasted_iota(jnp.int32, (pair, half), 1)
    by_row = lane < half // 2
    low = lax.rem(lax.broadcasted_iota(jnp.int32, (1, half), 1), 2 * quarter) < quarter
    factor = half ** (-0.5) * LOG2E

    def angles(blocks):
        found = []
        for row_table, col_table in ((row_cos, col_cos), (row_sin, col_sin)):
            found.append(
                jnp.concatenate(
                    [
                        jnp.where(by_row, row_table[pl.ds(s * chips + b, 1), :], col_table[...])
                        for b in blocks
                    ],
                    axis=0,
                )
            )
        return found

    def turn(raw, cos, sin, scale=None):
        parts = []
        for i in range(head // half):
            v = raw[:, i * half : (i + 1) * half].astype(jnp.bfloat16).astype(jnp.float32)
            other = jnp.where(low, pltpu.roll(v, half - quarter, 1), pltpu.roll(v, quarter, 1))
            turned = v * cos + other * sin
            if scale is not None:
                turned = turned * scale
            parts.append(turned.astype(jnp.bfloat16))
        return jnp.concatenate(parts, axis=1)

    def from_partner(b):
        for part in range(2):
            token_copy(2, b, 1 - c, part).wait_recv()

    def ask(i, blocks):
        first_row, n = q_parts[i]
        at = slice(first_row, first_row + n)
        cos, sin = angles(blocks)
        found = jnp.dot(
            normed[ctx_rows + first_row : ctx_rows + first_row + n, :],
            wq[...],
            preferred_element_type=jnp.float32,
        )
        found = turn(found, cos, sin, factor)

        @pl.when(own_kind)
        def _():
            queries[at, :] = found

        @pl.when(other_kind)
        def _():
            q_stage[at, :] = found
            q_copy(i).start()

    from_partner(z)
    locals_[2].wait()
    normalise(context_tokens, 0, 0, ctx_rows, 1)
    normalise(tokens, z * pair, ctx_rows, pair, 0)
    for i in (3, 4, 5):
        locals_[i].wait()
    cos, sin = angles([z])
    found = jnp.dot(normed[: sizes[0], :], wk[...], preferred_element_type=jnp.float32)
    keys = jnp.concatenate([found[:ctx_rows].astype(jnp.bfloat16), turn(found[ctx_rows:], cos, sin)], axis=0)
    values = jnp.dot(normed[: sizes[0], :], wv[...], preferred_element_type=jnp.float32).astype(jnp.bfloat16)
    hand_out(0, keys, values)
    forward(1, False)
    relay(0, (0, 2))
    relay(1, (0, 2))

    def process(d, carry):
        left = ring(z - d, chips)
        right = ring(z + d, chips)

        from_partner(left)
        from_partner(right)

        @pl.when(d == 2)
        def _():
            relay(1, (0, 4))

        @pl.when(d == 3)
        def _():
            relay(1, (1, 4))

        base = starts[1] + (d - 1) * 2 * pair
        normalise(tokens, left * pair, base, pair, 0)
        normalise(tokens, right * pair, base + pair, pair, 0)

        @pl.when(d == 1)
        def _():
            forward(2, True)

        @pl.when(d == 2)
        def _():
            forward(3, True)

        @pl.when(d == 3)
        def _():
            opposite = ring(z + far, chips)
            token_copy(2, opposite, c, 0).wait_recv()
            token_copy(2, opposite, c, 0).start()

        cos, sin = angles([left, right])
        v = normed[aligned(base, 2 * pair), :]
        keys = turn(jnp.dot(v, wk[...], preferred_element_type=jnp.float32), cos, sin)
        values = jnp.dot(v, wv[...], preferred_element_type=jnp.float32).astype(jnp.bfloat16)
        for g in (1, 2, 3):
            pl.when(d == g)(functools.partial(hand_out, g, keys, values))

        @pl.when(d == 1)
        def _():
            relay(0, (0, 3))
            relay(1, (0, 3))
            forward(2, False)
            relay(0, (1, 2))
            relay(1, (1, 2))

        @pl.when(d == 3)
        def _():
            relay(1, (2, 3))

        @pl.when(d == 2)
        def _():
            relay(0, (1, 3))
            relay(1, (1, 3))
            around = [z]
            for k in (1, 2):
                around += [ring(z - k, chips), ring(z + k, chips)]
            ask(0, around)
            relay(0, (0, 4), (2, 2))
            relay(1, (2, 2))
            forward(3, False)

        return carry

    lax.fori_loop(1, 4, process, 0)

    opposite = ring(z + far, chips)
    token_copy(2, opposite, c, 1).wait_recv()
    token_copy(2, opposite, c, 1).start()
    relay(0, (3, 2))
    relay(1, (3, 2))
    from_partner(opposite)
    normalise(tokens, opposite * pair, starts[4], pair, 0)
    relay(0, (1, 4))
    relay(1, (0, 5))
    cos, sin = angles([opposite])
    v = normed[starts[4] : starts[4] + pair, :]
    keys = turn(jnp.dot(v, wk[...], preferred_element_type=jnp.float32), cos, sin)
    values = jnp.dot(v, wv[...], preferred_element_type=jnp.float32).astype(jnp.bfloat16)
    hand_out(4, keys, values)
    relay(0, (2, 3))
    ask(1, [ring(z - 3, chips), ring(z + 3, chips), opposite])
    relay(0, (4, 2), (0, 5))
    relay(1, (2, 4), (4, 2), (3, 3))

    peak[...] = jnp.full(peak.shape, -jnp.inf, jnp.float32)
    total_weight[...] = jnp.zeros(total_weight.shape, jnp.float32)
    mixed[...] = jnp.zeros(mixed.shape, jnp.float32)

    def await_queries(i):
        @pl.when(other_kind)
        def _():
            awaited(queries.at[aligned(*q_parts[i])], q_sem.at[i])

    my_head = 2 * z + p
    weight_of_second = mod_pieces[my_head, 6:7, 0:1]
    lifted = mod_pieces[my_head, 7:8, 0:1] * LOG2E

    def attend(base, count, first_row, n, raised=None):
        keys_at = aligned(base, count)
        at = aligned(first_row, n)
        scores = [
            lax.dot_general(
                queries[at, m * half : (m + 1) * half],
                keys_values[keys_at, m * half : (m + 1) * half],
                (((1,), (1,)), ((), ())),
                preferred_element_type=jnp.float32,
            )
            for m in range(2)
        ]
        for m in range(2):
            score = scores[m] if raised is None else scores[m] + raised
            old = peak[m, at, :]
            new = jnp.maximum(old, jnp.max(score, axis=1, keepdims=True))
            alpha = jnp.exp2(old - new)
            weights = jnp.exp2(score - new[:, :1])
            total_weight[m, at, :] = total_weight[m, at, :] * alpha + jnp.sum(
                weights, axis=1, keepdims=True
            )
            peak[m, at, :] = new
            mixed[m, at, :] = mixed[m, at, :] * alpha[:, :1] + jnp.dot(
                weights.astype(jnp.bfloat16),
                keys_values[keys_at, head:],
                preferred_element_type=jnp.float32,
            )

    def out_copy(i, first_row, n):
        return remote(
            out_stage.at[first_row : first_row + n],
            attended.at[first_row : first_row + n],
            out_sem.at[3],
            out_sem.at[i],
            x + 1 - 2 * p,
            y,
            z,
            1 - c,
        )

    tiles = ((7 * pair, pair), (5 * pair, 2 * pair), q_parts[0])

    def finish(i):
        first_row, n = tiles[i]
        at = slice(first_row, first_row + n)
        diff = mixed[0, at, :] / total_weight[0, at, :1] - weight_of_second * (
            mixed[1, at, :] / total_weight[1, at, :1]
        )
        mean = jnp.sum(diff * diff, axis=1, keepdims=True) * (1.0 / head)
        found = (diff * lax.rsqrt(mean + EPSILON) * gain[...]).astype(jnp.bfloat16)

        @pl.when(own_kind)
        def _():
            attended[at, :] = found

        @pl.when(other_kind)
        def _():
            out_stage[at, :] = found
            out_copy(i, first_row, n).start()

    count = sp_size * sizes[0]
    column = lax.broadcasted_iota(jnp.int32, (1, count), 1)
    on_context = (column < sp_size * halves[0][0]) & (lax.rem(column, halves[0][0]) < ctx_rows)
    raised = jnp.where(on_context, lifted, 0.0)
    tile = block_tokens // 2

    await_queries(0)
    complete(0)

    def first_group(i, carry):
        attend(0, count, i * tile, tile, raised)

        @pl.when(i == 0)
        def _():
            await_queries(1)
            relay(0, (3, 3), (1, 5))
            relay(1, (1, 5), (4, 3))

        return carry

    lax.fori_loop(0, 2, first_group, 0)
    relay(0, (2, 4), (4, 3))
    relay(1, (3, 4))
    complete(1)

    def groups(j, carry):
        g = lax.div(j, 2) + 1
        i = lax.rem(j, 2)
        attend(sp_size * (starts[1] + (g - 1) * sizes[1]), sp_size * sizes[1], i * tile, tile)

        @pl.when(j == 0)
        def _():
            relay(0, (3, 4))
            relay(1, (4, 4))

        @pl.when(j == 1)
        def _():
            relay(0, (2, 5), (4, 4))
            relay(1, (2, 5))
            complete(2)

        @pl.when(j == 2)
        def _():
            relay(0, (3, 5))
            relay(1, (3, 5))

        return carry

    lax.fori_loop(0, 4, groups, 0)
    relay(0, (4, 5))
    relay(1, (4, 5))
    complete(3)
    locals_[6].wait()
    base = sp_size * starts[3]
    count = sp_size * sizes[3]
    rest = sp_size * sizes[4]
    attend(base, count, *q_parts[1])
    complete(4)
    for i in range(2):
        attend(base + count, rest, *tiles[i])
        finish(i)
    attend(base, count, *tiles[2])

    span = width // 2
    chunk = 1024

    def pair_copy(u):
        ref = pair_send.at[u]
        return remote(ref, pair_recv.at[u], ps_sem.at[0], pr_sem.at[u], x, y, z, 1 - c)

    def ring_copy(side, d, part):
        u = 2 * d + part
        into = (from_left, from_right)[side]
        sem = (left_sem, right_sem)[side]
        to = (ring(z + 1, chips), ring(z - 1, chips))[side]
        v = 2 * (d - 1) + part
        return remote(
            ring_stage.at[side, u], into.at[v], st_sem.at[side], sem.at[v], x, y, to, c
        )

    def ring_arrived(side, d, part):
        v = 2 * d + part
        into = (from_left, from_right)[side]
        sem = (left_sem, right_sem)[side]
        awaited(into.at[v], sem.at[v])

    def block_of(side, d):
        if d == 0:
            return 0
        if d == far:
            return 2 * far - 1
        return 2 * d if side == 0 else 2 * d - 1

    def compute(d):
        blocks = [block_of(0, d)] if d in (0, far) else [block_of(1, d), block_of(0, d)]
        others = [attended[aligned(j * pair + (1 - c) * rows, rows), :] for j in blocks]
        mines = [attended[aligned(j * pair + c * rows, rows), :] for j in blocks]
        both = jnp.concatenate(others + mines, axis=0)
        n = len(blocks)
        for part in range(2):
            for k in range(span // chunk):
                found = jnp.dot(
                    both,
                    wo[:, part * span + k * chunk : part * span + (k + 1) * chunk],
                    preferred_element_type=jnp.float32,
                )
                cols = slice(k * chunk, (k + 1) * chunk)
                for i, j in enumerate(blocks):
                    pair_send[2 * j + part, :, cols] = found[i * rows : (i + 1) * rows].astype(jnp.bfloat16)
                    own[2 * j + part, :, cols] = found[(n + i) * rows : (n + i + 1) * rows]
            for j in blocks:
                pair_copy(2 * j + part).start()

    def combine(side, d, part):
        u = 2 * block_of(side, d) + part
        pair_copy(u).wait_recv()
        value = own[u] + pair_recv[u].astype(jnp.float32)
        if not (d == far or (d == far - 1 and part != side)):
            ring_arrived(side, d, part)
            value = value + (from_left, from_right)[side][2 * d + part].astype(jnp.float32)
        ring_stage[side, 2 * d + part] = value.astype(jnp.bfloat16)
        ring_copy(side, d, part).start()

    def await_attended(i):
        @pl.when(other_kind)
        def _():
            awaited(attended.at[aligned(*tiles[i])], out_sem.at[i])

    await_attended(0)
    compute(4)
    combine(0, 4, 0)
    combine(1, 4, 1)
    await_attended(1)
    compute(3)
    combine(0, 3, 1)
    combine(1, 3, 0)
    attend(base + count, rest, *tiles[2])
    finish(2)
    combine(0, 3, 0)
    combine(1, 3, 1)

    await_attended(2)
    compute(2)
    combine(0, 2, 1)
    combine(1, 2, 0)
    compute(1)

    awaited(tokens.at[0 : 2 * (2 * far - 1) * part_rows + block_tokens // 2], tok_send.at[0])
    awaited(mod_parts.at[0 : sp_size - 1], part_sem.at[0])
    awaited(mod_pieces.at[0 : tp_size - 1], piece_sem.at[0])
    combine(0, 2, 0)
    combine(1, 2, 1)
    compute(0)
    first_rows = sum(h[0] for h in halves)
    second_rows = sum(h[1] for h in halves)
    for core in range(2):
        for cond, kind in ((own_kind, 0), (other_kind, 1)):

            @pl.when((c == core) & cond)
            def _():
                alone = (first_rows, second_rows)[core]
                away = (first_rows, second_rows)[1 - core]
                own_sends, later = ((2, 27), (3, 29))[core]
                once = away + (own_sends if kind == 0 else 2) * alone
                handed_on = (1 if core == 0 and kind == 1 else 2) * alone
                awaited(keys_values.at[0:once], kv_send.at[0])
                awaited(keys_values.at[0:handed_on], kv_send.at[1])
                awaited(keys_values.at[0 : later * alone], kv_send.at[2])

    @pl.when(other_kind)
    def _():
        awaited(queries, q_sem.at[2])
        awaited(attended, out_sem.at[3])

    awaited(pair_send, ps_sem.at[0])
    combine(0, 1, 1)
    combine(1, 1, 0)
    combine(0, 1, 0)
    combine(1, 1, 1)

    for part in (1, 0):
        cols = slice(part * span, (part + 1) * span)
        pair_copy(part).wait_recv()
        value = own[part] + pair_recv[part].astype(jnp.float32)
        ring_arrived(0, 0, part)
        value = value + from_left[part].astype(jnp.float32)
        ring_arrived(1, 0, part)
        value = value + from_right[part].astype(jnp.float32)
        result[:, cols] = (
            tokens[aligned(t * rows, rows), cols].astype(jnp.float32) + mod_rows[4:5, cols] * value
        ).astype(jnp.bfloat16)

    for side in range(2):
        awaited(ring_stage.at[side, 0 : 2 * far - 1], st_sem.at[side])


def tables(half):
    quarter = half // 4
    inverse = (ROPE_BASE ** (-np.arange(quarter, dtype=np.float32) / quarter)).astype(np.float32)
    inverse = np.tile(inverse, 4)
    sign = np.where(np.arange(half) % (2 * quarter) < quarter, -1.0, 1.0).astype(np.float32)
    found = []
    for count in (8192 // GRID_W, GRID_W):
        angle = np.arange(count, dtype=np.float32)[:, None] * inverse[None, :]
        found.append(np.cos(angle).astype(np.float32))
        found.append((np.sin(angle) * sign).astype(np.float32))
    return found


def shards(
    sp_size,
    tp_size,
    latent,
    context,
    condition,
    context_condition,
    modulation,
    query_weight,
    key_weight,
    value_weight,
    lambdas,
    context_lift,
    head_gain,
    output_weight,
):
    rows, width = latent.shape
    chips = tp_size // 2
    head = query_weight.shape[1]
    half = head // 2
    pair = 2 * rows
    block_tokens = rows * tp_size
    ctx_rows = context.shape[0]
    piece = modulation.shape[2]
    vmem = pl.BlockSpec(memory_space=pltpu.VMEM)
    smem = pl.BlockSpec(memory_space=pltpu.SMEM)
    anywhere = pl.BlockSpec(memory_space=pl.ANY)
    bf16, f32 = jnp.bfloat16, jnp.float32
    dma = pltpu.SemaphoreType.DMA
    blocks = (2 * chips, rows, width // 2)
    row_cos, row_sin, col_cos, col_sin = tables(half)
    return pl.pallas_call(
        functools.partial(kernel, sp_size, tp_size),
        out_shape=jax.ShapeDtypeStruct((rows, width), bf16),
        in_specs=[anywhere] * 2 + [vmem] * 2 + [anywhere] * 4 + [vmem] * 4 + [smem] * 2 + [vmem, anywhere],
        out_specs=vmem,
        scratch_shapes=[
            pltpu.VMEM((block_tokens, width), bf16),
            pltpu.VMEM(context.shape, bf16),
            pltpu.VMEM((ctx_rows + block_tokens, width), bf16),
            pltpu.VMEM(modulation.shape, bf16),
            pltpu.VMEM((width, head), bf16),
            pltpu.VMEM((width, head), bf16),
            pltpu.VMEM((width, head), bf16),
            pltpu.VMEM((head, width), bf16),
            pltpu.VMEM((sp_size * (ctx_rows + block_tokens), 2 * head), bf16),
            pltpu.VMEM((SIDE * block_tokens // 2, 2 * head), bf16),
            pltpu.VMEM((ctx_rows + block_tokens, 2 * head), bf16),
            pltpu.VMEM((block_tokens, head), bf16),
            pltpu.VMEM((block_tokens, head), bf16),
            pltpu.VMEM((2, block_tokens, 128), f32),
            pltpu.VMEM((2, block_tokens, 128), f32),
            pltpu.VMEM((2, block_tokens, head), f32),
            pltpu.VMEM((block_tokens, head), bf16),
            pltpu.VMEM((block_tokens, head), bf16),
            pltpu.VMEM((sp_size, 8, piece), f32),
            pltpu.VMEM((tp_size, 8, piece), f32),
            pltpu.VMEM((8, width), f32),
            pltpu.VMEM(blocks, f32),
            pltpu.VMEM(blocks, bf16),
            pltpu.VMEM(blocks, bf16),
            pltpu.VMEM((2, chips + 2, rows, width // 2), bf16),
            pltpu.VMEM((chips, rows, width // 2), bf16),
            pltpu.VMEM((chips, rows, width // 2), bf16),
            pltpu.VMEM((5 * pair, 2 * head), bf16),
            dma((7,)),
            dma((1,)),
            dma((2 * tp_size,)),
            dma((2,)),
            dma((2,)),
            dma((3,)),
            dma((5, 3)),
            dma((5,)),
            dma((5,)),
            dma((5,)),
            dma((3,)),
            dma((4,)),
            dma((1,)),
            dma((2 * chips,)),
            dma((2,)),
            dma((chips,)),
            dma((chips,)),
        ],
        compiler_params=pltpu.CompilerParams(
            collective_id=0, has_side_effects=True, vmem_limit_bytes=VMEM_LIMIT
        ),
        name="layer",
    )(
        latent,
        context,
        condition.reshape(1, -1),
        context_condition.reshape(1, -1),
        modulation,
        query_weight,
        key_weight,
        value_weight,
        jnp.asarray(row_cos),
        jnp.asarray(row_sin),
        jnp.asarray(col_cos),
        jnp.asarray(col_sin),
        lambdas,
        context_lift,
        head_gain.reshape(1, -1),
        output_weight,
    )


def solution(mesh):
    in_specs = (
        P(("sp", "tp"), None),
        P("sp", None),
        P(),
        P(),
        P(None, "sp", "tp"),
        P(None, "tp"),
        P(None, "tp"),
        P(None, "tp"),
        P("tp"),
        P("tp"),
        P(),
        P("tp", None),
    )
    out_specs = P(("sp", "tp"), None)
    body = functools.partial(shards, mesh.shape["sp"], mesh.shape["tp"])
    return jax.shard_map(body, mesh=mesh, in_specs=in_specs, out_specs=out_specs, check_vma=False)
```
